512 devices in a mesh: ep: 32 (over z, x), tp: 16 (over y, core).
Axes of the slice: x: 4, y: 8, z: 8, core: 2. Of those that a mesh axis runs over, the one named last changes fastest.
Arguments:
- queries: bfloat16 [16384, 1024], P('ep', 'tp'), may hold values from -6 to 6
- key_input: bfloat16 [16384, 256], P('ep'), may hold values from -6 to 6
- value_input: bfloat16 [16384, 256], P('ep'), may hold values from -6 to 6
- query_gain: float32 [64], replicated, may hold values from 0.1 to 1.9
- key_gain: float32 [64], replicated, may hold values from 0.1 to 1.9
- mix_out_weight: bfloat16 [1024, 2048], P('tp'), may hold values from -0.1875 to 0.1875
- expert_input: bfloat16 [5120, 2048], P('ep'), may hold values from -6 to 6
- ffn_gain: float32 [2048], replicated, may hold values from 0.1 to 1.9
- routes: int32 [5120, 2], P('ep'), may hold values from 0 to 31, all different within a row; in each aligned block of 160 rows (0 to 159, 160 to 319, ...) at most 15 rows name the same one
- route_scores: float32 [5120, 2], P('ep'), may hold values from 0.1 to 1
- gate_weight: bfloat16 [32, 2048, 4096], P('ep', None, 'tp'), may hold values from -0.125 to 0.125
- up_weight: bfloat16 [32, 2048, 4096], P('ep', None, 'tp'), may hold values from -0.125 to 0.125
- down_weight: bfloat16 [32, 4096, 2048], P('ep', 'tp'), may hold values from -0.09375 to 0.09375
Outputs:
- mixed_rows: bfloat16 [16384, 2048], P(('ep', 'tp'))
- expert_out: bfloat16 [5120, 2048], P('ep', 'tp')
The draws below stay inside these ranges and needn't reach their ends.
Inputs may be any that keep to these rules, and one draw needn't show every extreme that they name: `routes`: each row names 2 different experts. Within the rows of one index of ep (aligned blocks of 160 rows) no expert is named by more than 15 rows, and in every draw some expert is named by exactly 15 rows of some block.
All inputs are finite; a program needn't handle non-finite values.
Results may differ from the reference program's by a relative error of at most 0.019.
The reference program's roundings to bfloat16 on the way count: a program that leaves them out, or rounds other values in their place, can miss the bound.
Values may be sent and summed in bfloat16 or wider, within the bound.
A program may use at most 64 MiB of HBM per device.

```python
import math
import jax
import jax.numpy as jnp
import numpy as np
from jax import lax

D = 2048
HEADS = 16
KV_HEADS = 4
HD = 64
GRID_W = 64
FF = 4096
TOPK = 2
TOK2 = 160
EXPERTS = 32
CAP = 15
TOKENS1 = 16384
TOKENS2 = 5120
N_EP = 32
N_TP = 16


def block_levels(rng, dims, shards, least, top_value):
    loudness = 1.0
    for dim, parts in shards:
        heights = jax.random.uniform(jax.random.fold_in(jax.random.fold_in(rng, 6), dim), (parts,), jnp.float32, least / len(shards), top_value / len(shards))
        loudness = loudness * jnp.repeat(jnp.exp(heights), dims[dim] // parts).reshape((-1,) + (1,) * (len(dims) - 1 - dim))
    return loudness


def routed_block(stream_key, own, number, rows, number_of, top, most, skew):
    order = jax.random.permutation(stream_key, number_of)
    crowded, usual = portions_of(number_of, rows * top, most, skew, True), portions_of(number_of, rows * top, most, skew, False)
    places = jnp.arange(number_of)

    def named(tallies, rotation):
        used = int((tallies > 0).sum())
        fixed = max(1, used // 4)
        passed = fixed + (places - fixed + rotation * (used - fixed)) % max(1, number_of - fixed)
        return jnp.zeros((number_of,), jnp.int32).at[order[jnp.where(places < fixed, places, passed)]].set(jnp.asarray(tallies, jnp.int32))

    tallies = jnp.where(number % 4 == 0, named(crowded, number // 4), named(usual, number - number // 4 - 1))
    mixed = jax.random.permutation(jax.random.fold_in(own, 3), number_of)
    donor, taker = mixed[0:number_of // 2 * 2:2], mixed[1:number_of // 2 * 2:2]
    margin = jnp.minimum(tallies[donor] - 1, most - tallies[taker]) // 2
    margin = jnp.where((donor == order[0]) | (taker == order[0]) | (tallies[taker] == 0), 0, jnp.maximum(margin, 0))
    passed = jax.random.randint(jax.random.fold_in(own, 4), (number_of // 2,), 0, 1 << 20) % (margin + 1)
    tallies = tallies.at[donor].add(-passed).at[taker].add(passed)
    items = jnp.searchsorted(jnp.cumsum(tallies), jnp.arange(rows * top), side="right").astype(jnp.int32)
    listing = items.reshape(top, rows).T
    listing = listing[jax.random.permutation(jax.random.fold_in(own, 1), rows)]
    rotation = jax.random.randint(jax.random.fold_in(own, 2), (rows, 1), 0, top)
    return jnp.take_along_axis(listing, (jnp.arange(top)[None, :] + rotation) % top, axis=1)


def portions_of(count, total, bound, skew, full):
    loads = [(1 << 20) // math.isqrt(rank ** skew) + 1 for rank in range(1, count + 1)]
    largest = bound if full else min(bound, max(-(-total // count), total * loads[0] // sum(loads)))
    least = 1 if total - largest >= count - 1 else 0
    given, spare = [largest] + [least] * (count - 1), total - largest - least * (count - 1)
    while spare > 0:
        movable = [i for i in range(1, count) if given[i] < largest] or [i for i in range(1, count) if given[i] < bound]
        whole, budget = sum([loads[i] for i in movable]), spare
        for i in movable:
            more = min(bound - given[i], max(1, budget * loads[i] // whole), spare)
            given[i] = given[i] + more
            spare = spare - more
    return np.array(given)


def noise(key, extent, deviation, bound, cuts=(), kind=jnp.bfloat16):
    factor_of = block_levels(key, extent, cuts, -0.22, 0.18) if cuts else 1.0
    array = jax.random.normal(key, extent, jnp.float32) * deviation * factor_of
    return jnp.minimum(jnp.maximum(array, -bound), bound).astype(kind)


def setup_inputs(seed: int = 0) -> dict:
    streams_of = jax.random.split(jax.random.key(seed), 14)
    queries = noise(streams_of[0], (TOKENS1, HEADS * HD), 1.0, 6.0, ((0, 32), (1, 16)))
    key_input = noise(streams_of[1], (TOKENS1, KV_HEADS * HD), 1.0, 6.0, ((0, 32),))
    value_input = noise(streams_of[2], (TOKENS1, KV_HEADS * HD), 1.0, 6.0, ((0, 32),))
    query_gain = jnp.clip(1.0 + 0.18 * jax.random.normal(streams_of[3], (HD,), jnp.float32), 0.1, 1.9)
    key_gain = jnp.clip(1.0 + 0.18 * jax.random.normal(streams_of[4], (HD,), jnp.float32), 0.1, 1.9)
    mix_out_weight = noise(streams_of[5], (HEADS * HD, D), (HEADS * HD) ** -0.5, 0.1875, ((0, 16),))
    expert_input = noise(streams_of[6], (TOKENS2, D), 1.0, 6.0, ((0, 32),))
    ffn_gain = jnp.clip(1.0 + 0.18 * jax.random.normal(streams_of[7], (D,), jnp.float32), 0.1, 1.9)
    routes_keys = jax.random.split(jax.random.fold_in(streams_of[8], 1), TOKENS2 // TOK2)
    routes_turns = jax.random.permutation(jax.random.fold_in(streams_of[8], 3), TOKENS2 // TOK2)
    routes = jax.vmap(lambda own, number: routed_block(jax.random.fold_in(streams_of[8], 2), own, number, TOK2, EXPERTS, TOPK, CAP, 2))(routes_keys, routes_turns).reshape((TOKENS2, TOPK))
    route_scores = jnp.clip(jnp.exp(math.log(1.0) - 2.3025851 * jax.random.uniform(streams_of[9], (TOKENS2, TOPK), jnp.float32) ** block_levels(streams_of[9], (TOKENS2, TOPK), ((0, 32),), -0.2, 0.2)), 0.1, 1.0)
    gate_weight = noise(streams_of[10], (EXPERTS, D, FF), D ** -0.5, 0.125, ((0, 32), (2, 16)))
    up_weight = noise(streams_of[11], (EXPERTS, D, FF), D ** -0.5, 0.125, ((0, 32), (2, 16)))
    down_weight = noise(streams_of[12], (EXPERTS, FF, D), FF ** -0.5, 0.09375, ((0, 32), (1, 16)))
    return dict(queries=queries, key_input=key_input, value_input=value_input, query_gain=query_gain, key_gain=key_gain, mix_out_weight=mix_out_weight, expert_input=expert_input, ffn_gain=ffn_gain, routes=routes, route_scores=route_scores, gate_weight=gate_weight, up_weight=up_weight, down_weight=down_weight)


EPSILON = 1e-06
ROPE_BASE = 10000.0

def rotate_half(portion, cos_table, sin_table):
    front_half, back_half = jnp.split(portion, 2, axis=-1)
    cos_table = cos_table[:, None, :]
    sin_table = sin_table[:, None, :]
    return jnp.concatenate([front_half * cos_table - back_half * sin_table, back_half * cos_table + front_half * sin_table], axis=-1)

def prepare(source, channel_gain, positions):
    token_count = source.shape[0]
    values_f = source.astype(jnp.float32).reshape(token_count, -1, HD)
    normed = values_f * lax.rsqrt(lax.optimization_barrier(jnp.mean(values_f * values_f, axis=-1, keepdims=True)) + EPSILON) * channel_gain
    quarter = HD // 4
    inverse = ROPE_BASE ** (-jnp.arange(quarter, dtype=jnp.float32) / quarter)
    row_angle = (positions // GRID_W).astype(jnp.float32)[:, None] * inverse[None, :]
    col_angle = (positions % GRID_W).astype(jnp.float32)[:, None] * inverse[None, :]
    half_width = HD // 2
    turned = jnp.concatenate([rotate_half(normed[..., :half_width], jnp.cos(row_angle), jnp.sin(row_angle)), rotate_half(normed[..., half_width:], jnp.cos(col_angle), jnp.sin(col_angle))], axis=-1)
    return turned.reshape(token_count, -1).astype(jnp.bfloat16)

def attend_head(head_args):
    query_head, key_head, value_head = head_args
    length = query_head.shape[0]
    key_span = math.gcd(length, 512)
    query_blocks = query_head.reshape(length // key_span, key_span, HD)

    def one_block(query_block):
        scores = jnp.dot(query_block, key_head.T, preferred_element_type=jnp.float32) * HD ** (-0.5)
        weights = jnp.exp(scores)
        weighted = jnp.dot(weights.astype(jnp.bfloat16), value_head, preferred_element_type=jnp.float32)
        return (weighted / lax.optimization_barrier(jnp.sum(weights, axis=-1, keepdims=True))).astype(jnp.bfloat16)
    return lax.map(one_block, query_blocks).reshape(length, HD)

def reference(queries, key_input, value_input, query_gain, key_gain, mix_out_weight, expert_input, ffn_gain, routes, route_scores, gate_weight, up_weight, down_weight):
    length = queries.shape[0]
    positions = jnp.arange(length, dtype=jnp.int32)
    group_size = HEADS // KV_HEADS
    q_rot = prepare(queries, query_gain, positions).reshape(length, HEADS, HD).transpose(1, 0, 2)
    k_rot = prepare(key_input, key_gain, positions).reshape(length, KV_HEADS, HD).transpose(1, 0, 2)
    v_heads = value_input.reshape(length, KV_HEADS, HD).transpose(1, 0, 2)
    attended = lax.map(attend_head, (q_rot, jnp.repeat(k_rot, group_size, axis=0), jnp.repeat(v_heads, group_size, axis=0)))
    attended = attended.transpose(1, 0, 2).reshape(length, HEADS * HD)
    col_width = HEADS * HD // N_TP

    def add_group(running_sum, group_index):
        start_col = (group_index * col_width).astype(jnp.int32)
        columns = lax.dynamic_slice_in_dim(attended, start_col, col_width, 1)
        weight_rows = lax.dynamic_slice_in_dim(mix_out_weight, start_col, col_width, 0)
        portion = jnp.dot(columns, weight_rows, preferred_element_type=jnp.float32).astype(jnp.bfloat16)
        portion = lax.optimization_barrier(portion)
        return (running_sum + portion.astype(jnp.float32), None)
    mixed_sum, _ = lax.scan(add_group, jnp.zeros((length, D), jnp.float32), jnp.arange(N_TP, dtype=jnp.int32))
    mixed_rows = mixed_sum.astype(jnp.bfloat16)
    tokens = expert_input.shape[0]
    flat_routes = routes.reshape(N_EP, TOK2 * TOPK)
    hit_table = (flat_routes[:, :, None] == jnp.arange(EXPERTS, dtype=jnp.int32)[None, None, :]).astype(jnp.int32)
    position = lax.optimization_barrier(jnp.sum((jnp.cumsum(hit_table, axis=1) - hit_table) * hit_table, axis=-1))
    per_expert = N_EP * CAP
    slot_index = flat_routes * per_expert + jnp.arange(N_EP, dtype=jnp.int32)[:, None] * CAP + position
    slot_index = slot_index.reshape(-1).astype(jnp.int32)
    pair_token = jnp.arange(tokens * TOPK, dtype=jnp.int32) // TOPK
    owner_row = jnp.full((EXPERTS * per_expert,), tokens, jnp.int32).at[slot_index].set(pair_token)
    padded = jnp.concatenate([expert_input, jnp.zeros((1, D), jnp.bfloat16)], axis=0)
    buffers = padded[owner_row].reshape(EXPERTS, per_expert, D)
    ff_width = FF // N_TP

    def run_expert(expert_args):
        slot_rows, w_gate, w_up, w_down = expert_args
        values_f = slot_rows.astype(jnp.float32)
        row_scale = lax.rsqrt(lax.optimization_barrier(jnp.mean(values_f * values_f, axis=-1, keepdims=True)) + EPSILON)
        scaled = (values_f * ffn_gain).astype(jnp.bfloat16)
        gate_pre = row_scale * jnp.dot(scaled, w_gate, preferred_element_type=jnp.float32)
        up_pre = row_scale * jnp.dot(scaled, w_up, preferred_element_type=jnp.float32)
        hidden = (jax.nn.silu(gate_pre) * up_pre).astype(jnp.bfloat16)
        running_sum = jnp.zeros((per_expert, D), jnp.float32)
        for group_index in range(N_TP):
            lower = group_index * ff_width
            portion = jnp.dot(hidden[:, lower:lower + ff_width], w_down[lower:lower + ff_width], preferred_element_type=jnp.float32).astype(jnp.bfloat16)
            running_sum = running_sum + lax.optimization_barrier(portion).astype(jnp.float32)
        return running_sum.astype(jnp.bfloat16)
    pair_rows = lax.map(run_expert, (buffers, gate_weight, up_weight, down_weight)).reshape(-1, D)
    route_weight = route_scores / lax.optimization_barrier(jnp.sum(route_scores, axis=-1, keepdims=True))
    picked = pair_rows[slot_index].astype(jnp.float32).reshape(tokens, TOPK, D)
    expert_out = lax.optimization_barrier(jnp.sum(picked * route_weight[:, :, None], axis=1)).astype(jnp.bfloat16)
    return (mixed_rows, expert_out)
```

```python
import functools
import math
from types import SimpleNamespace

import jax
import jax.numpy as jnp
import numpy as np
from jax import lax
from jax.experimental import pallas as pl
from jax.experimental.pallas import tpu as pltpu
from jax.sharding import PartitionSpec as P

HD = 64
GRID_W = 64
EPSILON = 1e-06
ROPE_BASE = 10000.0
SLOTS = 16
MESH = pl.DeviceIdType.MESH
F32 = jnp.float32
BF16 = jnp.bfloat16


def angle_tables(rows):
    quarter = HD // 4
    inverse = (ROPE_BASE ** (-np.arange(quarter, dtype=np.float32) / quarter)).astype(np.float32)
    lane = np.arange(2 * HD)
    freq = inverse[lane % quarter]
    is_row = (lane % HD) < HD // 2
    sign = np.where((lane // quarter) % 2 == 0, -1.0, 1.0).astype(np.float32)

    def table(count, keep):
        angle = (np.arange(count, dtype=np.float32)[:, None] * freq[None, :]).astype(np.float32)
        cos = np.where(keep, np.cos(angle), 0.0).astype(np.float32)
        sin = np.where(keep, np.sin(angle) * sign, 0.0).astype(np.float32)
        return cos, sin

    return table(rows, is_row) + table(GRID_W, ~is_row)


def kernel(
    g,
    kqv,
    key_gain,
    query_gain,
    row_cos,
    row_sin,
    col_cos,
    col_sin,
    tokens,
    routes,
    scores,
    ffn_gain,
    mix_w,
    gate_w,
    up_w,
    down_w,
    mixed_out,
    expert_out,
    kv,
    q_own,
    q_all,
    o_acc,
    o_in,
    att_out,
    att_in,
    att_row,
    w_all,
    tok_own,
    outbound,
    slots,
    wg,
    wu,
    wd,
    gate_acc,
    up_acc,
    sq_acc,
    hidden,
    ring_out,
    ring_in,
    rows_out,
    rows_in,
    hot,
    sem_local,
    sem_kv_s,
    sem_kv_r,
    sem_kvf_s,
    sem_kvf_r,
    sem_q_s,
    sem_q_r,
    sem_o_s,
    sem_o_r,
    sem_a_s,
    sem_a_r,
    sem_w_s,
    sem_w_r,
    sem_wf_s,
    sem_wf_r,
    sem_ex_s,
    sem_ex_r,
    sem_d_s,
    sem_d_r,
    sem_b_s,
    sem_b_r,
    sem_c_s,
    sem_c_r,
    sem_r_s,
    sem_r_r,
):
    nz, nx, ny, ep, tp = g.nz, g.nx, g.ny, g.nz * g.nx, g.ny * 2
    half_ep = ep // 2
    me_e, me_t = lax.axis_index("ep"), lax.axis_index("tp")
    z, x = me_e // nx, me_e % nx
    y, c = me_t // 2, me_t % 2
    sib = me_t + 1 - 2 * c
    own_half = me_e // half_ep
    tq, tok, d, ff = g.tq, g.tok, g.d, g.ff
    feat = d // 4
    par = y % 2

    def send(src, dst, ssem, rsem, to_e, to_t):
        return pltpu.make_async_remote_copy(
            src_ref=src, dst_ref=dst, send_sem=ssem, recv_sem=rsem,
            device_id=(to_e, to_t), device_id_type=MESH,
        )

    def arrived(dst, rsem):
        send(dst, dst, rsem, rsem, me_e, sib).wait_recv()

    def left(src, ssem):
        send(src, src, ssem, ssem, me_e, sib).wait_send()

    def al(v, m):
        return pl.multiple_of(v, m)

    barrier = pltpu.get_barrier_semaphore()

    def greet_plane(i, _):
        pl.semaphore_signal(barrier, inc=1, device_id=((me_e + i) % ep, me_t), device_id_type=MESH)
        pl.semaphore_signal(barrier, inc=1, device_id=((me_e + i) % ep, sib), device_id_type=MESH)
        return 0

    def greet_line(i, _):
        pl.semaphore_signal(barrier, inc=1, device_id=(me_e, (me_t + i) % tp), device_id_type=MESH)
        return 0

    lax.fori_loop(1, ep, greet_plane, 0)
    lax.fori_loop(1, tp, greet_line, 0)

    feat_at = al((par * 2 + c) * feat, feat)
    loads = [
        pltpu.make_async_copy(tokens.at[:, pl.ds(feat_at, feat)], tok_own, sem_local.at[0]),
        pltpu.make_async_copy(mix_w, w_all.at[pl.ds(al(me_t * HD, HD), HD)], sem_local.at[1]),
        pltpu.make_async_copy(gate_w.at[0], wg.at[c], sem_local.at[2]),
        pltpu.make_async_copy(up_w.at[0], wu.at[c], sem_local.at[3]),
        pltpu.make_async_copy(down_w.at[0], wd.at[pl.ds(al(c * ff, ff), ff)], sem_local.at[4]),
    ]
    for copy in loads:
        copy.start()

    r0, r1 = routes[:, 0:1], routes[:, 1:2]
    lanes_e = lax.broadcasted_iota(jnp.int32, (tok, ep), 1)
    hit0 = (lanes_e == r0).astype(F32)
    hit1 = (lanes_e == r1).astype(F32)
    before = (
        lax.broadcasted_iota(jnp.int32, (tok, tok), 1) < lax.broadcasted_iota(jnp.int32, (tok, tok), 0)
    ).astype(BF16)
    count = jnp.dot(before, (hit0 + hit1).astype(BF16), preferred_element_type=F32)
    pos0 = jnp.sum(count * hit0, axis=1, keepdims=True).astype(jnp.int32)
    pos1 = jnp.sum(count * hit1, axis=1, keepdims=True).astype(jnp.int32)
    lanes_s = lax.broadcasted_iota(jnp.int32, (tok, ep * SLOTS), 1)
    hot[0] = (lanes_s == r0 * SLOTS + pos0).astype(BF16)
    hot[1] = (lanes_s == r1 * SLOTS + pos1).astype(BF16)
    loads[0].wait()
    outbound[...] = lax.dot_general(
        hot[0] + hot[1], tok_own[...], (((0,), (0,)), ((), ())), preferred_element_type=F32
    ).astype(BF16)

    lane = lax.broadcasted_iota(jnp.int32, (GRID_W, 2 * HD), 1)
    low = lane < HD
    is_u = (lane // (HD // 4)) % 2 == 0
    gain = jnp.concatenate([key_gain[...], query_gain[...]], axis=1)
    blocks = tq // GRID_W
    row_at = me_e * blocks
    for b in range(blocks):
        at = b * GRID_W
        v = kqv[at : at + GRID_W, 0 : 2 * HD].astype(F32)
        sq = v * v
        s_low = jnp.sum(jnp.where(low, sq, 0.0), axis=1, keepdims=True)
        s_high = jnp.sum(jnp.where(low, 0.0, sq), axis=1, keepdims=True)
        scale = jnp.where(low, lax.rsqrt(s_low * (1.0 / HD) + EPSILON), lax.rsqrt(s_high * (1.0 / HD) + EPSILON))
        n = v * scale * gain
        cos = col_cos[...] + row_cos[pl.ds(row_at + b, 1), :]
        sin = col_sin[...] + row_sin[pl.ds(row_at + b, 1), :]
        swapped = jnp.where(is_u, pltpu.roll(n, 2 * HD - HD // 4, 1), pltpu.roll(n, HD // 4, 1))
        turned = n * cos + swapped * sin
        kv[z, at : at + GRID_W, :] = jnp.where(
            low, turned, kqv[at : at + GRID_W, 2 * HD : 4 * HD].astype(F32)
        ).astype(BF16)
        att_row[at : at + GRID_W, :] = turned
    q_own[...] = jnp.transpose(att_row[...])[HD : 2 * HD, :].astype(BF16)

    pl.semaphore_wait(barrier, 2 * (ep - 1) + tp - 1)

    slot_at = al((me_e % half_ep) * SLOTS, SLOTS)
    to_core = y * 2 + own_half

    def dispatch(i, start):
        to_e = (me_e + i) % ep
        return send(
            outbound.at[pl.ds(al(to_e * SLOTS, SLOTS), SLOTS)],
            slots.at[pl.ds(slot_at, SLOTS), pl.ds(feat_at, feat)],
            sem_d_s.at[i], sem_d_r.at[(me_e % half_ep) * 2 + c], to_e, to_core,
        )

    dispatch_self = pltpu.make_async_copy(
        outbound.at[pl.ds(al(me_e * SLOTS, SLOTS), SLOTS)],
        slots.at[pl.ds(slot_at, SLOTS), pl.ds(feat_at, feat)],
        sem_d_r.at[(me_e % half_ep) * 2 + c],
    )

    def dispatch_start(i, _):
        dispatch(i, True).start()
        return 0

    lax.fori_loop(1, ep, dispatch_start, 0)

    @pl.when(c == own_half)
    def _():
        dispatch_self.start()

    @pl.when(c != own_half)
    def _():
        dispatch(0, True).start()

    def q_copy(i):
        return send(q_own, q_all.at[x], sem_q_s.at[i], sem_q_r.at[x], z * nx + (x + i) % nx, me_t)

    q_self = pltpu.make_async_copy(q_own, q_all.at[x], sem_q_r.at[x])
    q_self.start()
    for i in range(1, nx):
        q_copy(i).start()

    hq = tq // 2
    kv_mine = pl.ds(al(c * hq, hq), hq)
    kv_other = pl.ds(al((1 - c) * hq, hq), hq)

    def kv_copy(i):
        return send(
            kv.at[z, kv_mine], kv.at[z, kv_mine], sem_kv_s.at[i], sem_kv_r.at[z], ((z + i) % nz) * nx + x, me_t
        )

    order = sorted(range(1, nz), key=lambda i: (min(i, nz - i), i))
    for i in order:
        kv_copy(i).start()

    for copy in loads[1:]:
        copy.wait()

    extra = [
        send(wg.at[c], wg.at[c], sem_ex_s.at[0], sem_ex_r.at[0], me_e, sib),
        send(wu.at[c], wu.at[c], sem_ex_s.at[1], sem_ex_r.at[1], me_e, sib),
        send(
            wd.at[pl.ds(al(c * ff, ff), ff)], wd.at[pl.ds(al(c * ff, ff), ff)],
            sem_ex_s.at[2], sem_ex_r.at[2], me_e, sib,
        ),
    ]
    for copy in extra:
        copy.start()

    half_y = ny // 2
    right = ((y + 1) % ny) * 2 + c
    leftward = ((y + ny - 1) % ny) * 2 + c

    def w_block(yy, core):
        return w_all.at[pl.ds(al((yy * 2 + core) * HD, HD), HD)]

    def w_right(s):
        b = w_block((y + ny - s) % ny, c)
        return send(b, b, sem_w_s.at[0, s], sem_w_r.at[0, s], me_e, right)

    def w_left(s):
        b = w_block((y + s) % ny, c)
        return send(b, b, sem_w_s.at[1, s], sem_w_r.at[1, s], me_e, leftward)

    def w_twin(yy):
        b = w_block(yy, c)
        return send(b, b, sem_wf_s.at[yy], sem_wf_r.at[yy], me_e, sib)

    def w_step(s):
        if s > 0:
            from_left = (y + ny - s) % ny
            arrived(w_block(from_left, c), sem_w_r.at[0, s - 1])
            w_twin(from_left).start()
            if s < half_y:
                from_right = (y + s) % ny
                arrived(w_block(from_right, c), sem_w_r.at[1, s - 1])
                w_twin(from_right).start()
        else:
            w_twin(y).start()
        if s < half_y:
            w_right(s).start()
        if s < half_y - 1:
            w_left(s).start()

    score_scale = HD ** (-0.5) * math.log2(math.e)
    kt = min(256, tq)

    def kv_ready(i):
        if i == 0:
            return
        zz = (z + nz - i) % nz
        arrived(kv.at[zz, kv_mine], sem_kv_r.at[zz])
        send(kv.at[zz, kv_mine], kv.at[zz, kv_mine], sem_kvf_s.at[zz], sem_kvf_r.at[zz], me_e, sib).start()

    def attend(i):
        zz = (z + nz - i) % nz
        if i:
            arrived(kv.at[zz, kv_other], sem_kvf_r.at[zz])
        rows = lax.broadcasted_iota(jnp.int32, (80, tq), 0)
        vt = jnp.where(rows < 16, 1.0, jnp.transpose(kv[zz].astype(F32))[48:128, :]).astype(BF16)

        def one(xx, _):
            total = None
            for k in range(tq // kt):
                s_t = jnp.dot(kv[zz, k * kt : (k + 1) * kt, 0:HD], q_all[xx], preferred_element_type=F32)
                p = jnp.exp2(s_t * score_scale).astype(BF16)
                part = jnp.dot(vt[:, k * kt : (k + 1) * kt], p, preferred_element_type=F32)
                total = part if total is None else total + part
            if i:
                o_acc[xx] = o_acc[xx] + total
            else:
                o_acc[xx] = total
            return 0

        lax.fori_loop(0, nx, one, 0)

    def q_ready():
        def one(i, _):
            arrived(q_all.at[i], sem_q_r.at[i])
            return 0

        lax.fori_loop(0, nx, one, 0)

    own_at, other_at = par * (d // 2), (1 - par) * (d // 2)

    def swap(k):
        at = al(own_at + k * feat, feat)
        b = slots.at[:, pl.ds(at, feat)]
        return send(b, b, sem_b_s.at[k], sem_b_r.at[k], me_e, leftward if k == 0 else right)

    def slots_ready():
        for core in range(2):
            at = al(own_at + core * feat, feat)

            def one(j, _):
                arrived(
                    slots.at[pl.ds(al(j * SLOTS, SLOTS), SLOTS), pl.ds(at, feat)], sem_d_r.at[j * 2 + core]
                )
                return 0

            lax.fori_loop(0, half_ep, one, 0)
            swap(core).start()

    def half_products(start, first):
        for k in range(2):
            at = al(start + k * feat, feat)
            v = slots[:, pl.ds(at, feat)].astype(F32)
            sq = jnp.sum(v * v, axis=1, keepdims=True)
            scaled = (v * ffn_gain[:, pl.ds(at, feat)]).astype(BF16)
            for core in range(2):
                gp = jnp.dot(scaled, wg[core, pl.ds(at, feat), :], preferred_element_type=F32)
                up = jnp.dot(scaled, wu[core, pl.ds(at, feat), :], preferred_element_type=F32)
                if first and k == 0:
                    gate_acc[core], up_acc[core] = gp, up
                else:
                    gate_acc[core], up_acc[core] = gate_acc[core] + gp, up_acc[core] + up
            if first and k == 0:
                sq_acc[...] = jnp.broadcast_to(sq, sq_acc.shape)
            else:
                sq_acc[...] = sq_acc[...] + sq

    def ffn_first():
        for k in range(2):
            arrived(wg.at[1 - c], sem_ex_r.at[0]) if k == 0 else arrived(wu.at[1 - c], sem_ex_r.at[1])
        arrived(wd.at[pl.ds(al((1 - c) * ff, ff), ff)], sem_ex_r.at[2])
        half_products(own_at, True)

    def ffn_second():
        for k in range(2):
            arrived(slots.at[:, pl.ds(al(other_at + k * feat, feat), feat)], sem_b_r.at[k])
        half_products(other_at, False)
        scale = lax.rsqrt(sq_acc[:, 0:1] * (1.0 / d) + EPSILON)
        for core in range(2):
            gate = scale * gate_acc[core]
            hidden[:, core * ff : (core + 1) * ff] = (
                gate / (1.0 + jnp.exp(-gate)) * (scale * up_acc[core])
            ).astype(BF16)

    yb = d // ny
    n_slots = half_ep * SLOTS
    hs = n_slots // 2

    def partial_of(dest):
        return jnp.dot(hidden[...], wd[:, pl.ds(al(dest * yb, yb), yb)], preferred_element_type=F32)

    def ring_copy(way, s):
        rows = pl.ds(0, hs if s == 0 else n_slots)
        return send(
            ring_out.at[way, s, rows], ring_in.at[way, s, rows], sem_c_s.at[way, s], sem_c_r.at[way, s],
            me_e, right if way == 0 else leftward,
        )

    def ring_ready(way, s):
        arrived(ring_in.at[way, s, pl.ds(0, hs if s == 0 else n_slots)], sem_c_r.at[way, s])

    def ring_step(s):
        if s == 0:
            block = partial_of((y + half_y) % ny)
            ring_out[0, 0, 0:hs] = block[0:hs].astype(BF16)
            ring_copy(0, 0).start()
            ring_out[1, 0, 0:hs] = block[hs:].astype(BF16)
            ring_copy(1, 0).start()
            return
        for way in range(2):
            dest = (y + half_y - s) % ny if way == 0 else (y + ny - half_y + s) % ny
            block = partial_of(dest)
            ring_ready(way, s - 1)
            if s == 1:
                mine = pl.ds(0, hs) if way == 0 else pl.ds(hs, hs)
                lo, hi = block[0:hs], block[hs:]
                if way == 0:
                    lo = lo + ring_in[0, 0, 0:hs].astype(F32)
                else:
                    hi = hi + ring_in[1, 0, 0:hs].astype(F32)
                ring_out[way, s, 0:hs] = lo.astype(BF16)
                ring_out[way, s, hs:] = hi.astype(BF16)
            else:
                ring_out[way, s] = (block + ring_in[way, s - 1].astype(F32)).astype(BF16)
            ring_copy(way, s).start()

    def back_copy(j, core):
        src_e = c * half_ep + j
        return send(
            rows_out.at[core, pl.ds(al(j * SLOTS, SLOTS), SLOTS)],
            rows_in.at[pl.ds(al(me_e * SLOTS, SLOTS), SLOTS)],
            sem_r_s.at[j, core], sem_r_r.at[me_e], src_e, y * 2 + core,
        )

    def back_self(j, core):
        return pltpu.make_async_copy(
            rows_out.at[core, pl.ds(al(j * SLOTS, SLOTS), SLOTS)],
            rows_in.at[pl.ds(al(me_e * SLOTS, SLOTS), SLOTS)],
            sem_r_r.at[me_e],
        )

    def ring_end():
        s = half_y - 1
        block = partial_of(y)
        for way in range(2):
            ring_ready(way, s)
        if s == 0:
            lo = block[0:hs] + ring_in[0, 0, 0:hs].astype(F32)
            hi = block[hs:] + ring_in[1, 0, 0:hs].astype(F32)
            block = jnp.concatenate([lo, hi], axis=0)
        else:
            block = block + ring_in[0, s].astype(F32) + ring_in[1, s].astype(F32)
        block = block.astype(BF16)
        for core in range(2):
            rows_out[core] = block[:, core * (yb // 2) : (core + 1) * (yb // 2)]

        def one(j, _):
            for core in range(2):
                here = (c * half_ep + j == me_e) & (c == core)

                @pl.when(here)
                def _():
                    back_self(j, core).start()

                @pl.when(jnp.logical_not(here))
                def _():
                    back_copy(j, core).start()

            return 0

        lax.fori_loop(0, half_ep, one, 0)

    def combine():
        def one(j, _):
            arrived(rows_in.at[pl.ds(al(j * SLOTS, SLOTS), SLOTS)], sem_r_r.at[j])
            return 0

        lax.fori_loop(0, ep, one, 0)
        s0, s1 = scores[:, 0:1], scores[:, 1:2]
        whole = s0 + s1
        p0 = jnp.dot(hot[0], rows_in[...], preferred_element_type=F32)
        p1 = jnp.dot(hot[1], rows_in[...], preferred_element_type=F32)
        expert_out[...] = (p0 * (s0 / whole) + p1 * (s1 / whole)).astype(BF16)

    def o_copy(i):
        to_x = (x + i) % nx
        return send(
            o_acc.at[to_x, pl.ds(8, 72)], o_in.at[x], sem_o_s.at[i], sem_o_r.at[x], z * nx + to_x, me_t
        )

    def o_send():
        for i in range(1, nx):
            o_copy(i).start()

    rows_t = tq // tp
    ht = rows_t // 2

    def a_copy(i):
        to_t = (me_t + i) % tp
        return send(
            att_out.at[pl.ds(al(to_t * ht, ht), ht)], att_in.at[pl.ds(al(me_t * ht, ht), ht)],
            sem_a_s.at[i], sem_a_r.at[me_t], me_e, to_t,
        )

    a_self = pltpu.make_async_copy(
        att_out.at[pl.ds(al(me_t * ht, ht), ht)], att_in.at[pl.ds(al(me_t * ht, ht), ht)], sem_a_r.at[me_t]
    )

    def attend_end():
        total = o_acc[x][8:80]
        for i in range(1, nx):
            xx = (x + i) % nx
            arrived(o_in.at[xx], sem_o_r.at[xx])
            total = total + o_in[xx]
        att_t = total[8:72] / total[0:1]
        att = jnp.transpose(jnp.concatenate([att_t, att_t], axis=0))[:, 0:HD]
        for t in range(tp):
            at = t * rows_t
            att_out[t * ht : (t + 1) * ht, :] = jnp.concatenate(
                [att[at : at + ht], att[at + ht : at + rows_t]], axis=1
            ).astype(BF16)
        a_self.start()

        def one(i, _):
            a_copy(i).start()
            return 0

        lax.fori_loop(1, tp, one, 0)

    def project():
        def one(j, _):
            arrived(att_in.at[pl.ds(al(j * ht, ht), ht)], sem_a_r.at[j])
            return 0

        lax.fori_loop(0, tp, one, 0)

        def two(yy, _):
            arrived(w_block(yy, 1 - c), sem_wf_r.at[yy])
            return 0

        lax.fori_loop(0, ny, two, 0)
        pieces = []
        for j in range(tp // 2):
            a = att_in[2 * j * ht : (2 * j + 1) * ht, :]
            b = att_in[(2 * j + 1) * ht : (2 * j + 2) * ht, :]
            top = jnp.concatenate([a[:, 0:HD], b[:, 0:HD]], axis=1)
            low_rows = jnp.concatenate([a[:, HD:], b[:, HD:]], axis=1)
            pieces.append(jnp.concatenate([top, low_rows], axis=0))
        lhs = jnp.concatenate(pieces, axis=1)
        mixed_out[...] = jnp.dot(lhs, w_all[...], preferred_element_type=F32).astype(BF16)

    w_step(0)
    q_ready()
    attend(0)
    work = order
    after = {}
    plan = g.plan(half_y, len(work))
    actions = dict(
        slots=slots_ready, ffn1=ffn_first, ffn2=ffn_second, ring_end=ring_end, o_send=o_send,
        attend_end=attend_end, project=project, combine=combine,
    )
    for name, arg in plan:
        if name == "kv":
            kv_ready(work[arg])
        elif name == "attend":
            attend(work[arg])
        elif name == "w":
            w_step(arg)
        elif name == "ring":
            ring_step(arg)
        else:
            actions[name]()

    def sent_dispatch(i, _):
        left(outbound.at[pl.ds(0, SLOTS)], sem_d_s.at[i])
        return 0

    lax.fori_loop(1, ep, sent_dispatch, 0)

    @pl.when(c != own_half)
    def _():
        left(outbound.at[pl.ds(0, SLOTS)], sem_d_s.at[0])

    for i in range(1, nx):
        q_copy(i).wait_send()
        o_copy(i).wait_send()
    for i in order:
        kv_copy(i).wait_send()
        zz = (z + nz - i) % nz
        left(kv.at[zz, kv_mine], sem_kvf_s.at[zz])
    for copy in extra:
        copy.wait_send()
    for s in range(half_y):
        w_right(s).wait_send()
        if s < half_y - 1:
            w_left(s).wait_send()
        for way in range(2):
            ring_copy(way, s).wait_send()
    for k in range(2):
        swap(k).wait_send()

    def sent_w(yy, _):
        left(w_block(yy, c), sem_wf_s.at[yy])
        return 0

    lax.fori_loop(0, ny, sent_w, 0)

    def sent_back(j, _):
        for core in range(2):
            here = (c * half_ep + j == me_e) & (c == core)

            @pl.when(jnp.logical_not(here))
            def _():
                left(rows_out.at[core, pl.ds(0, SLOTS)], sem_r_s.at[j, core])

        return 0

    lax.fori_loop(0, half_ep, sent_back, 0)

    def sent_a(i, _):
        left(att_out.at[pl.ds(0, ht)], sem_a_s.at[i])
        return 0

    lax.fori_loop(1, tp, sent_a, 0)


def default_plan(half_y, shards):
    kv = [("kv", i) for i in range(shards)]
    at = [("attend", i) for i in range(shards)]
    plan = [("slots", 0)]
    plan += [("w", s) for s in range(1, half_y + 1)]
    for a, b in zip(kv, at):
        plan += [a, b]
    plan += [("o_send", 0), ("ffn1", 0), ("ffn2", 0)]
    plan += [("ring", s) for s in range(half_y)]
    plan += [("attend_end", 0), ("ring_end", 0), ("project", 0), ("combine", 0)]
    return plan


def local(g, queries, key_input, value_input, query_gain, key_gain, mix_out_weight, expert_input, ffn_gain,
          routes, route_scores, gate_weight, up_weight, down_weight):
    ep, tp = g.nz * g.nx, g.ny * 2
    kv_at = (lax.axis_index("tp") * g.kv_heads // tp) * HD
    own_k = lax.dynamic_slice_in_dim(key_input, kv_at, HD, 1)
    own_v = lax.dynamic_slice_in_dim(value_input, kv_at, HD, 1)
    kqv = jnp.concatenate([own_k, queries, own_v, own_v], axis=1)
    tables = angle_tables(ep * g.tq // GRID_W)
    half_slots = ep // 2 * SLOTS
    vmem = pl.BlockSpec(memory_space=pltpu.VMEM)
    hbm = pl.BlockSpec(memory_space=pl.ANY)
    yb = g.d // g.ny
    half_y = g.ny // 2
    dma = pltpu.SemaphoreType.DMA
    return pl.pallas_call(
        functools.partial(kernel, g),
        out_shape=(
            jax.ShapeDtypeStruct((g.tq // tp, g.d), BF16),
            jax.ShapeDtypeStruct((g.tok, g.d // tp), BF16),
        ),
        in_specs=[vmem] * 7 + [hbm] + [vmem] * 3 + [hbm] * 4,
        out_specs=(vmem, vmem),
        scratch_shapes=[
            pltpu.VMEM((g.nz, g.tq, 2 * HD), BF16),
            pltpu.VMEM((HD, g.tq), BF16),
            pltpu.VMEM((g.nx, HD, g.tq), BF16),
            pltpu.VMEM((g.nx, 80, g.tq), F32),
            pltpu.VMEM((g.nx, 72, g.tq), F32),
            pltpu.VMEM((g.tq // 2, 2 * HD), BF16),
            pltpu.VMEM((g.tq // 2, 2 * HD), BF16),
            pltpu.VMEM((g.tq, 2 * HD), F32),
            pltpu.VMEM((tp * HD, g.d), BF16),
            pltpu.VMEM((g.tok, g.d // 4), BF16),
            pltpu.VMEM((ep * SLOTS, g.d // 4), BF16),
            pltpu.VMEM((half_slots, g.d), BF16),
            pltpu.VMEM((2, g.d, g.ff), BF16),
            pltpu.VMEM((2, g.d, g.ff), BF16),
            pltpu.VMEM((2 * g.ff, g.d), BF16),
            pltpu.VMEM((2, half_slots, g.ff), F32),
            pltpu.VMEM((2, half_slots, g.ff), F32),
            pltpu.VMEM((half_slots, 128), F32),
            pltpu.VMEM((half_slots, 2 * g.ff), BF16),
            pltpu.VMEM((2, half_y, half_slots, yb), BF16),
            pltpu.VMEM((2, half_y, half_slots, yb), BF16),
            pltpu.VMEM((2, half_slots, yb // 2), BF16),
            pltpu.VMEM((ep * SLOTS, yb // 2), BF16),
            pltpu.VMEM((2, g.tok, ep * SLOTS), BF16),
            dma((5,)),
            dma((g.nz,)), dma((g.nz,)), dma((g.nz,)), dma((g.nz,)),
            dma((g.nx,)), dma((g.nx,)), dma((g.nx,)), dma((g.nx,)),
            dma((tp,)), dma((tp,)),
            dma((2, half_y)), dma((2, half_y)), dma((g.ny,)), dma((g.ny,)),
            dma((3,)), dma((3,)),
            dma((ep,)), dma((ep,)),
            dma((2,)), dma((2,)),
            dma((2, half_y)), dma((2, half_y)),
            dma((ep // 2, 2)), dma((ep,)),
        ],
        compiler_params=pltpu.CompilerParams(
            collective_id=0, has_side_effects=True, vmem_limit_bytes=48 * 1024 * 1024
        ),
    )(
        kqv, key_gain.reshape(1, HD), query_gain.reshape(1, HD), *[jnp.asarray(t) for t in tables],
        expert_input, routes, route_scores, ffn_gain.reshape(1, g.d), mix_out_weight,
        gate_weight, up_weight, down_weight,
    )


SIZES = SimpleNamespace(nz=8, nx=4, ny=8, tq=512, tok=160, d=2048, ff=256, kv_heads=4, plan=default_plan)


def solution(mesh, g=SIZES):
    placed = (
        P("ep", "tp"),
        P("ep", None),
        P("ep", None),
        P(),
        P(),
        P("tp", None),
        P("ep", None),
        P(),
        P("ep", None),
        P("ep", None),
        P("ep", None, "tp"),
        P("ep", None, "tp"),
        P("ep", "tp", None),
    )
    return jax.shard_map(
        functools.partial(local, g),
        mesh=mesh,
        in_specs=placed,
        out_specs=(P(("ep", "tp"), None), P("ep", "tp")),
        check_vma=False,
    )
```

```python
import contextlib
import functools
import math
from types import SimpleNamespace

import jax
import jax.numpy as jnp
import numpy as np
from jax import lax
from jax.experimental import pallas as pl
from jax.experimental.pallas import tpu as pltpu
from jax.sharding import PartitionSpec as P

HD = 64
GRID_W = 64
EPSILON = 1e-06
ROPE_BASE = 10000.0
SLOTS = 16
CHUNKS = 4
MESH = pl.DeviceIdType.MESH
F32 = jnp.float32
BF16 = jnp.bfloat16
TRACE = False


def scope(name):
    return jax.named_scope(name) if TRACE else contextlib.nullcontext()


def angle_tables(rows):
    quarter = HD // 4
    inverse = (ROPE_BASE ** (-np.arange(quarter, dtype=np.float32) / quarter)).astype(np.float32)
    lane = np.arange(2 * HD)
    freq = inverse[lane % quarter]
    is_row = (lane % HD) < HD // 2
    sign = np.where((lane // quarter) % 2 == 0, -1.0, 1.0).astype(np.float32)

    def table(count, keep):
        angle = (np.arange(count, dtype=np.float32)[:, None] * freq[None, :]).astype(np.float32)
        cos = np.where(keep, np.cos(angle), 0.0).astype(np.float32)
        sin = np.where(keep, np.sin(angle) * sign, 0.0).astype(np.float32)
        return cos, sin

    return table(rows, is_row) + table(GRID_W, ~is_row)


def kernel(
    g,
    queries_h,
    keys_h,
    values_h,
    key_gain_h,
    query_gain_h,
    row_cos_h,
    row_sin_h,
    col_cos_h,
    col_sin_h,
    tokens,
    routes_h,
    scores_h,
    ffn_gain_h,
    mix_w,
    gate_w,
    up_w,
    down_w,
    mixed_out,
    expert_out,
    kv,
    q_own,
    q_all,
    o_acc,
    o_out,
    o_in,
    att_out,
    att_in,
    att_row,
    w_all,
    tok_own,
    outbound,
    slots,
    wg,
    wu,
    wd,
    gate_acc,
    up_acc,
    sq_acc,
    hidden,
    ring_out,
    ring_in,
    rows_out,
    rows_in,
    hot,
    share,
    ring_part,
    q_raw,
    k_raw,
    v_raw,
    key_gain,
    query_gain,
    row_cos,
    row_sin,
    col_cos,
    col_sin,
    routes,
    scores,
    ffn_gain,
    sem_local,
    sem_kv_s,
    sem_kv_r,
    sem_kvf_s,
    sem_kvf_r,
    sem_q_s,
    sem_q_r,
    sem_o_s,
    sem_o_r,
    sem_a_s,
    sem_a_r,
    sem_w_s,
    sem_w_r,
    sem_wf_s,
    sem_wf_r,
    sem_wx_s,
    sem_wx_r,
    sem_ex_s,
    sem_ex_r,
    sem_d_s,
    sem_d_r,
    sem_b_s,
    sem_b_r,
    sem_c_s,
    sem_c_r,
    sem_r_s,
    sem_r_r,
):
    nz, nx, ny, ep, tp = g.nz, g.nx, g.ny, g.nz * g.nx, g.ny * 2
    half_ep = ep // 2
    me_e, me_t = lax.axis_index("ep"), lax.axis_index("tp")
    z, x = me_e // nx, me_e % nx
    y, c = me_t // 2, me_t % 2
    sib = me_t + 1 - 2 * c
    own_half = me_e // half_ep
    tq, tok, d, ff = g.tq, g.tok, g.d, g.ff
    feat = d // 4
    par = y % 2

    def send(src, dst, ssem, rsem, to_e, to_t):
        return pltpu.make_async_remote_copy(
            src_ref=src, dst_ref=dst, send_sem=ssem, recv_sem=rsem,
            device_id=(to_e, to_t), device_id_type=MESH,
        )

    def arrived(dst, rsem):
        send(dst, dst, rsem, rsem, me_e, sib).wait_recv()

    def left(src, ssem):
        send(src, src, ssem, ssem, me_e, sib).wait_send()

    def al(v, m):
        return pl.multiple_of(v, m)

    barrier = pltpu.get_barrier_semaphore()

    def greet_plane(i, _):
        pl.semaphore_signal(barrier, inc=1, device_id=((me_e + i) % ep, me_t), device_id_type=MESH)
        pl.semaphore_signal(barrier, inc=1, device_id=((me_e + i) % ep, sib), device_id_type=MESH)
        return 0

    def greet_line(i, _):
        pl.semaphore_signal(barrier, inc=1, device_id=(me_e, (me_t + i) % tp), device_id_type=MESH)
        return 0

    lax.fori_loop(1, ep, greet_plane, 0)
    lax.fori_loop(1, tp, greet_line, 0)

    feat_at = al((par * 2 + c) * feat, feat)
    dh = d // 2
    col_half = x % 2
    cols_mine = pl.ds(al(col_half * dh, dh), dh)
    cols_other = pl.ds(al((1 - col_half) * dh, dh), dh)
    blocks = tq // GRID_W
    head = me_t * g.kv_heads // tp
    head_at = al((head // 2) * 2 * HD, 2 * HD) if g.kv_heads > 1 else 0
    head_lanes = pl.ds(head_at, 2 * HD) if g.kv_heads > 1 else pl.ds(0, HD)
    kv_lanes = slice(0, 2 * HD) if g.kv_heads > 1 else slice(0, HD)
    pairs = [
        (routes_h, routes),
        (scores_h, scores),
        (tokens.at[:, pl.ds(feat_at, feat)], tok_own),
        (queries_h, q_raw),
        (keys_h.at[:, head_lanes], k_raw.at[:, kv_lanes]),
        (values_h.at[:, head_lanes], v_raw.at[:, kv_lanes]),
        (key_gain_h, key_gain),
        (query_gain_h, query_gain),
        (row_cos_h.at[pl.ds(me_e * blocks, blocks)], row_cos),
        (row_sin_h.at[pl.ds(me_e * blocks, blocks)], row_sin),
        (col_cos_h, col_cos),
        (col_sin_h, col_sin),
        (mix_w.at[:, cols_mine], w_all.at[y, c, :, cols_mine]),
        (gate_w.at[0], wg.at[c]),
        (up_w.at[0], wu.at[c]),
        (down_w.at[0], wd.at[pl.ds(al(c * ff, ff), ff)]),
        (ffn_gain_h, ffn_gain),
    ]
    loads = [pltpu.make_async_copy(a, b, sem_local.at[i]) for i, (a, b) in enumerate(pairs)]
    for copy in loads:
        copy.start()

    for copy in loads[0:2]:
        copy.wait()
    r0, r1 = routes[0:1, :], routes[1:2, :]
    rows_e = lax.broadcasted_iota(jnp.int32, (ep, tok), 0)
    hit0 = (rows_e == r0).astype(F32)
    hit1 = (rows_e == r1).astype(F32)
    before = (
        lax.broadcasted_iota(jnp.int32, (tok, tok), 0) < lax.broadcasted_iota(jnp.int32, (tok, tok), 1)
    ).astype(BF16)
    count = jnp.dot((hit0 + hit1).astype(BF16), before, preferred_element_type=F32)
    slot0 = r0 * SLOTS + jnp.sum(count * hit0, axis=0, keepdims=True).astype(jnp.int32)
    slot1 = r1 * SLOTS + jnp.sum(count * hit1, axis=0, keepdims=True).astype(jnp.int32)
    rows_s = lax.broadcasted_iota(jnp.int32, (ep * SLOTS, tok), 0)
    to_slots = ((rows_s == slot0) | (rows_s == slot1)).astype(BF16)
    loads[2].wait()
    outbound[...] = jnp.dot(to_slots, tok_own[...], preferred_element_type=F32).astype(BF16)

    lane = lax.broadcasted_iota(jnp.int32, (GRID_W, 2 * HD), 1)
    low = lane < HD
    is_u = (lane // (HD // 4)) % 2 == 0
    for copy in loads[3:12]:
        copy.wait()
    gain = jnp.concatenate([key_gain[...], query_gain[...]], axis=1)
    odd = head % 2 == 1
    q_wide = jnp.transpose(jnp.concatenate([q_raw[...], q_raw[...]], axis=0).astype(F32))
    if g.kv_heads > 1:
        k_all, v_all = k_raw[...].astype(F32), v_raw[...].astype(F32)
        k_wide = jnp.where(odd, pltpu.roll(k_all, HD, 1), k_all)
        v_wide = jnp.where(odd, v_all, pltpu.roll(v_all, HD, 1))
    else:
        k_wide = jnp.concatenate([k_raw[:, 0:HD]] * 2, axis=1).astype(F32)
        v_wide = jnp.concatenate([v_raw[:, 0:HD]] * 2, axis=1).astype(F32)
    for b in range(blocks):
        at = b * GRID_W
        v = jnp.where(low, k_wide[at : at + GRID_W], q_wide[at : at + GRID_W])
        sq = v * v
        s_low = jnp.sum(jnp.where(low, sq, 0.0), axis=1, keepdims=True)
        s_high = jnp.sum(jnp.where(low, 0.0, sq), axis=1, keepdims=True)
        scale = jnp.where(low, lax.rsqrt(s_low * (1.0 / HD) + EPSILON), lax.rsqrt(s_high * (1.0 / HD) + EPSILON))
        n = v * scale * gain
        cos = col_cos[...] + row_cos[b : b + 1, :]
        sin = col_sin[...] + row_sin[b : b + 1, :]
        swapped = jnp.where(is_u, pltpu.roll(n, 2 * HD - HD // 4, 1), pltpu.roll(n, HD // 4, 1))
        turned = n * cos + swapped * sin
        kv[z, at : at + GRID_W, :] = jnp.where(low, turned, v_wide[at : at + GRID_W]).astype(BF16)
        att_row[at : at + GRID_W, :] = turned
    q_own[...] = jnp.transpose(att_row[...])[HD : 2 * HD, :].astype(BF16)

    with scope("barrier"):
        pl.semaphore_wait(barrier, 2 * (ep - 1) + tp - 1)

    slot_at = al((me_e % half_ep) * SLOTS, SLOTS)
    to_core = y * 2 + own_half

    fw = feat // 2

    def wave_lanes(wave):
        return pl.ds(wave * fw, fw), pl.ds(al(feat_at + wave * fw, fw), fw)

    def dispatch(i, wave):
        to_e = (me_e + i) % ep
        return send(
            outbound.at[pl.ds(al(to_e * SLOTS, SLOTS), SLOTS), wave_lanes(wave)[0]],
            slots.at[pl.ds(slot_at, SLOTS), wave_lanes(wave)[1]],
            sem_d_s.at[wave, i], sem_d_r.at[wave, (me_e % half_ep) * 2 + c], to_e, to_core,
        )

    def dispatch_self(wave):
        return pltpu.make_async_copy(
            outbound.at[pl.ds(al(me_e * SLOTS, SLOTS), SLOTS), wave_lanes(wave)[0]],
            slots.at[pl.ds(slot_at, SLOTS), wave_lanes(wave)[1]],
            sem_d_r.at[wave, (me_e % half_ep) * 2 + c],
        )

    def q_copy(i):
        return send(q_own, q_all.at[x], sem_q_s.at[i], sem_q_r.at[x], z * nx + (x + i) % nx, me_t)

    q_all[x] = q_own[...]
    for i in range(1, nx):
        q_copy(i).start()

    hq = tq // 2
    kv_mine = pl.ds(al(c * hq, hq), hq)
    kv_other = pl.ds(al((1 - c) * hq, hq), hq)

    half_z = nz // 2
    way_c = 1 - 2 * c
    chain = [(way, m) for m in range(1, half_z + 1) for way in (1, -1) if way == 1 or m < half_z]

    def shard(way, m):
        return (z + nz - way * way_c * m) % nz

    def kv_pass(way, m):
        b = kv.at[shard(way, m), kv_mine]
        to_z = (z + nz + way * way_c) % nz
        at = 0 if way == 1 else 1
        return send(b, b, sem_kv_s.at[at, m], sem_kv_r.at[shard(way, m)], to_z * nx + x, me_t)

    def kv_passes(way, m):
        return m < half_z if way == 1 else m < half_z - 1

    for way in (1, -1):
        if kv_passes(way, 0):
            kv_pass(way, 0).start()

    near = ep // 4
    for wave in range(2):

        def dispatch_start(i, _):
            dispatch(i, wave).start()
            return 0

        lax.fori_loop(near, ep - near, dispatch_start, 0)
        lax.fori_loop(1, near, dispatch_start, 0)
        lax.fori_loop(ep - near, ep, dispatch_start, 0)

        @pl.when(c == own_half)
        def _():
            dispatch_self(wave).start()

        @pl.when(c != own_half)
        def _():
            dispatch(0, wave).start()

    for copy in loads[12:]:
        copy.wait()

    extra = [
        send(wg.at[c], wg.at[c], sem_ex_s.at[0], sem_ex_r.at[0], me_e, sib),
        send(wu.at[c], wu.at[c], sem_ex_s.at[1], sem_ex_r.at[1], me_e, sib),
        send(
            wd.at[pl.ds(al(c * ff, ff), ff)], wd.at[pl.ds(al(c * ff, ff), ff)],
            sem_ex_s.at[2], sem_ex_r.at[2], me_e, sib,
        ),
    ]

    def extra_start():
        for copy in extra:
            copy.start()

    half_y = ny // 2
    right = ((y + 1) % ny) * 2 + c
    leftward = ((y + ny - 1) % ny) * 2 + c
    ahead = ((y + ny + way_c) % ny) * 2 + c
    behind = ((y + ny - way_c) % ny) * 2 + c

    def w_block(s):
        return w_all.at[(y + ny + ny - way_c * s) % ny, c, :, cols_mine]

    def w_ahead(s):
        return send(w_block(s), w_block(s), sem_w_s.at[0, s], sem_w_r.at[0, s], me_e, ahead)

    def w_behind(s):
        return send(w_block(-s), w_block(-s), sem_w_s.at[1, s], sem_w_r.at[1, s], me_e, behind)

    def w_fresh(s):
        return [s] if s in (0, half_y) else [s, -s]

    def w_row(r):
        return (y + ny + ny - way_c * r) % ny

    def w_quarter(r, k, other):
        half = 1 - col_half if other else col_half
        return w_all.at[w_row(r), c, :, pl.ds(al(half * dh + k * (dh // 2), dh // 2), dh // 2)]

    def w_swap(r, k):
        to_x = (x + nx - 1) % nx if k == 0 else (x + 1) % nx
        q = w_quarter(r, k, False)
        return send(q, q, sem_wx_s.at[k, w_row(r)], sem_wx_r.at[k, w_row(r)], z * nx + to_x, me_t)

    def w_twin(r):
        b = w_block(r)
        return send(b, b, sem_wf_s.at[w_row(r)], sem_wf_r.at[w_row(r)], me_e, sib)

    def w_step(s):
        if s > 0:
            arrived(w_block(s), sem_w_r.at[0, s - 1])
            if s < half_y:
                arrived(w_block(-s), sem_w_r.at[1, s - 1])
        if s < half_y:
            w_ahead(s).start()
        if s < half_y - 1:
            w_behind(s).start()
        pending.extend(w_fresh(s))

    pending = []

    def w_exchange():
        for r in pending:
            for k in range(2):
                w_swap(r, k).start()
            w_twin(r).start()
        pending.clear()

    def w_far():
        b = w_all.at[:, c, :, cols_other]
        return send(b, b, sem_wf_s.at[ny], sem_wf_r.at[ny], me_e, sib)

    def w_end():
        for s in range(half_y + 1):
            for r in w_fresh(s):
                for k in range(2):
                    arrived(w_quarter(r, k, True), sem_wx_r.at[k, w_row(r)])
        w_far().start()

    def o_copy(j):
        to_x = (x + j) % nx
        return send(o_out.at[to_x], o_in.at[x], sem_o_s.at[j], sem_o_r.at[x], z * nx + to_x, me_t)

    score_scale = HD ** (-0.5) * math.log2(math.e)

    def kv_twin(way, m):
        zz = shard(way, m)
        return send(kv.at[zz, kv_mine], kv.at[zz, kv_mine], sem_kvf_s.at[zz], sem_kvf_r.at[zz], me_e, sib)

    def kv_ready(i):
        way, m = chain[i]
        zz = shard(way, m)
        arrived(kv.at[zz, kv_mine], sem_kv_r.at[zz])
        if kv_passes(way, m):
            kv_pass(way, m).start()
        kv_twin(way, m).start()

    def values_of(zz):
        rows = lax.broadcasted_iota(jnp.int32, (80, tq), 0)
        return jnp.where(rows < 16, 1.0, jnp.transpose(kv[zz].astype(F32))[48:128, :]).astype(BF16)

    def scores_of(zz, vt, xx):
        s_t = jnp.dot(kv[zz, :, 0:HD], q_all[xx], preferred_element_type=F32)
        p = jnp.exp2(s_t * score_scale).astype(BF16)
        return jnp.dot(vt, p, preferred_element_type=F32)

    def attend_own(part):
        vt = values_of(z)
        for j in range(nx) if part is None else ([0] if part == 0 else range(1, nx)):
            xx = (x + j) % nx
            if j:
                arrived(q_all.at[xx], sem_q_r.at[xx])
            o_acc[xx] = scores_of(z, vt, xx)

    def attend(i):
        last = i == len(chain) - 1
        zz = shard(*chain[i])
        arrived(kv.at[zz, kv_other], sem_kvf_r.at[zz])
        vt = values_of(zz)
        for j in range(1, nx + 1):
            xx = (x + j) % nx
            whole = o_acc[xx] + scores_of(zz, vt, xx)
            if last and j < nx:
                high = whole[0:8].astype(BF16)
                o_out[xx, 0:8] = high
                o_out[xx, 8:16] = (whole[8:16] - high.astype(F32)).astype(BF16)
                o_out[xx, 16:80] = whole[16:80].astype(BF16)
                o_copy(j).start()
            else:
                o_acc[xx] = whole

    own_at, other_at = par * (d // 2), (1 - par) * (d // 2)

    def swap(k, wave):
        at = al(own_at + k * feat + wave * fw, fw)
        b = slots.at[:, pl.ds(at, fw)]
        return send(b, b, sem_b_s.at[k, wave], sem_b_r.at[k, wave], me_e, leftward if k == 0 else right)

    def slots_ready(wave):
        for core in range(2):
            at = al(own_at + core * feat + wave * fw, fw)

            def one(j, _):
                arrived(
                    slots.at[pl.ds(al(j * SLOTS, SLOTS), SLOTS), pl.ds(at, fw)], sem_d_r.at[wave, j * 2 + core]
                )
                return 0

            lax.fori_loop(0, half_ep, one, 0)
            swap(core, wave).start()

    def half_products(start, first):
        for k in range(2):
            at = al(start + k * feat, feat)
            v = slots[:, pl.ds(at, feat)].astype(F32)
            sq = jnp.sum(v * v, axis=1, keepdims=True)
            scaled = (v * ffn_gain[:, pl.ds(at, feat)]).astype(BF16)
            for core in range(2):
                gp = jnp.dot(scaled, wg[core, pl.ds(at, feat), :], preferred_element_type=F32)
                up = jnp.dot(scaled, wu[core, pl.ds(at, feat), :], preferred_element_type=F32)
                if first and k == 0:
                    gate_acc[core], up_acc[core] = gp, up
                else:
                    gate_acc[core], up_acc[core] = gate_acc[core] + gp, up_acc[core] + up
            if first and k == 0:
                sq_acc[...] = jnp.broadcast_to(sq, sq_acc.shape)
            else:
                sq_acc[...] = sq_acc[...] + sq

    def ffn_first():
        for k in range(2):
            arrived(wg.at[1 - c], sem_ex_r.at[0]) if k == 0 else arrived(wu.at[1 - c], sem_ex_r.at[1])
        arrived(wd.at[pl.ds(al((1 - c) * ff, ff), ff)], sem_ex_r.at[2])
        half_products(own_at, True)

    def ffn_second():
        for k in range(2):
            for wave in range(2):
                arrived(slots.at[:, pl.ds(al(other_at + k * feat + wave * fw, fw), fw)], sem_b_r.at[k, wave])
        half_products(other_at, False)
        scale = lax.rsqrt(sq_acc[:, 0:1] * (1.0 / d) + EPSILON)
        for core in range(2):
            gate = scale * gate_acc[core]
            hidden[:, core * ff : (core + 1) * ff] = (
                gate / (1.0 + jnp.exp(-gate)) * (scale * up_acc[core])
            ).astype(BF16)
        ring_fill(0)

    yb = d // ny
    n_slots = half_ep * SLOTS
    hs = n_slots // 2

    def partial_of(dest):
        return jnp.dot(hidden[...], wd[:, pl.ds(al(dest * yb, yb), yb)], preferred_element_type=F32)

    cr = n_slots // CHUNKS

    def ring_has(way, s, k):
        return s > 0 or (k < CHUNKS // 2) == (way == 0)

    def ring_copy(way, s, k):
        rows = pl.ds(k * cr, cr)
        return send(
            ring_out.at[way, s, rows], ring_in.at[way, s, rows], sem_c_s.at[way, s, k], sem_c_r.at[way, s, k],
            me_e, right if way == 0 else leftward,
        )

    def ring_take(way, s, k, block):
        if not ring_has(way, s, k):
            return block
        rows = slice(k * cr, (k + 1) * cr)
        arrived(ring_in.at[way, s, pl.ds(k * cr, cr)], sem_c_r.at[way, s, k])
        return block + ring_in[way, s, rows].astype(F32)

    def ring_fill(s):
        for way in range(1 if s in (0, half_y) else 2):
            dest = (y + half_y - s) % ny if way == 0 else (y + ny - half_y + s) % ny
            ring_part[s % 2, way] = partial_of(dest)

    def ring_step(s):
        for j in range(CHUNKS):
            for way in range(2):
                k = (j + CHUNKS // 2) % CHUNKS if (s == 1 and way == 0) or (s != 1 and way == 1) else j
                if not ring_has(way, s, k):
                    continue
                rows = slice(k * cr, (k + 1) * cr)
                block = ring_part[s % 2, way if s else 0, rows]
                if s:
                    block = ring_take(way, s - 1, k, block)
                ring_out[way, s, rows] = block.astype(BF16)
                ring_copy(way, s, k).start()
        ring_fill(s + 1)

    def back_copy(j, core):
        src_e = c * half_ep + j
        return send(
            rows_out.at[core, pl.ds(al(j * SLOTS, SLOTS), SLOTS)],
            rows_in.at[pl.ds(al(me_e * SLOTS, SLOTS), SLOTS)],
            sem_r_s.at[j, core], sem_r_r.at[me_e], src_e, y * 2 + core,
        )

    def back_self(j, core):
        return pltpu.make_async_copy(
            rows_out.at[core, pl.ds(al(j * SLOTS, SLOTS), SLOTS)],
            rows_in.at[pl.ds(al(me_e * SLOTS, SLOTS), SLOTS)],
            sem_r_r.at[me_e],
        )

    def ring_end():
        s = half_y - 1

        def one(j, _):
            for core in range(2):
                here = (c * half_ep + j == me_e) & (c == core)

                @pl.when(here)
                def _():
                    back_self(j, core).start()

                @pl.when(jnp.logical_not(here))
                def _():
                    back_copy(j, core).start()

            return 0

        for k in range(CHUNKS):
            rows = slice(k * cr, (k + 1) * cr)
            block = ring_part[half_y % 2, 0, rows]
            for way in range(2):
                block = ring_take(way, s, k, block)
            block = block.astype(BF16)
            for core in range(2):
                rows_out[core, rows] = block[:, core * (yb // 2) : (core + 1) * (yb // 2)]
            per = half_ep // CHUNKS
            lax.fori_loop(k * per, (k + 1) * per, one, 0)

    def make_hot():
        fill = jnp.full((1, g.tok_pad - tok), -1, jnp.int32)
        rows = lax.broadcasted_iota(jnp.int32, (ep * SLOTS, g.tok_pad), 0)
        w0, w1 = scores[0:1, :], scores[1:2, :]
        whole = w0 + w1
        for k, (slot, w) in enumerate(((slot0, w0 / whole), (slot1, w1 / whole))):
            mask = (rows == jnp.concatenate([slot, fill], axis=1)).astype(F32)
            hot[k] = jnp.transpose(mask).astype(BF16)
            wide = jnp.concatenate([w, jnp.zeros((1, g.tok_pad - tok), F32)], axis=1)
            share[k] = jnp.transpose(jnp.broadcast_to(wide, (128, g.tok_pad)))

    def combine():
        def one(j, _):
            arrived(rows_in.at[pl.ds(al(j * SLOTS, SLOTS), SLOTS)], sem_r_r.at[j])
            return 0

        lax.fori_loop(0, ep, one, 0)
        p0 = jnp.dot(hot[0], rows_in[...], preferred_element_type=F32)
        p1 = jnp.dot(hot[1], rows_in[...], preferred_element_type=F32)
        expert_out[...] = (p0 * share[0] + p1 * share[1])[0:tok].astype(BF16)

    rows_t = tq // tp
    ht = rows_t // 2

    def a_copy(i):
        to_t = (me_t + i) % tp
        return send(
            att_out.at[pl.ds(al(to_t * ht, ht), ht)], att_in.at[pl.ds(al(me_t * ht, ht), ht)],
            sem_a_s.at[i], sem_a_r.at[me_t], me_e, to_t,
        )

    a_self = pltpu.make_async_copy(
        att_out.at[pl.ds(al(me_t * ht, ht), ht)], att_in.at[pl.ds(al(me_t * ht, ht), ht)], sem_a_r.at[me_t]
    )

    def attend_end():
        total = o_acc[x]
        numer, denom = total[16:80], total[0:8]
        for i in range(1, nx):
            xx = (x + i) % nx
            arrived(o_in.at[xx], sem_o_r.at[xx])
            numer = numer + o_in[xx, 16:80].astype(F32)
            denom = denom + o_in[xx, 0:8].astype(F32) + o_in[xx, 8:16].astype(F32)
        att_t = numer / denom[0:1]
        att = jnp.transpose(jnp.concatenate([att_t, att_t], axis=0))[:, 0:HD]
        for t in range(tp):
            at = t * rows_t
            att_out[t * ht : (t + 1) * ht, :] = jnp.concatenate(
                [att[at : at + ht], att[at + ht : at + rows_t]], axis=1
            ).astype(BF16)
        a_self.start()

        def one(i, _):
            a_copy(i).start()
            return 0

        lax.fori_loop(1, tp, one, 0)

    def project():
        def one(j, _):
            arrived(att_in.at[pl.ds(al(j * ht, ht), ht)], sem_a_r.at[j])
            return 0

        lax.fori_loop(0, tp, one, 0)

        for yy in range(ny):
            arrived(w_all.at[yy, 1 - c, :, cols_mine], sem_wf_r.at[yy])
        arrived(w_all.at[:, 1 - c, :, cols_other], sem_wf_r.at[ny])
        pieces = []
        for j in range(tp // 2):
            a = att_in[2 * j * ht : (2 * j + 1) * ht, :]
            b = att_in[(2 * j + 1) * ht : (2 * j + 2) * ht, :]
            top = jnp.concatenate([a[:, 0:HD], b[:, 0:HD]], axis=1)
            low_rows = jnp.concatenate([a[:, HD:], b[:, HD:]], axis=1)
            pieces.append(jnp.concatenate([top, low_rows], axis=0))
        lhs = jnp.concatenate(pieces, axis=1)
        mixed_out[...] = jnp.dot(lhs, w_all[...].reshape(tp * HD, d), preferred_element_type=F32).astype(BF16)

    w_step(0)
    plan = g.plan(half_y, len(chain))
    actions = dict(
        ffn1=ffn_first, ffn2=ffn_second, ring_end=ring_end,
        attend_end=attend_end, project=project, combine=combine, hot=make_hot, w_end=w_end, extra=extra_start, wx=w_exchange,
    )
    for name, arg in plan:
        with scope(name + str(arg)):
            if name == "kv":
                kv_ready(arg)
            elif name == "attend":
                attend(arg)
            elif name == "w":
                w_step(arg)
            elif name == "ring":
                ring_step(arg)
            elif name == "own":
                attend_own(arg)
            elif name == "slots":
                slots_ready(arg)
            else:
                actions[name]()

    for wave in range(2):

        def sent_dispatch(i, _):
            left(outbound.at[pl.ds(0, SLOTS), pl.ds(0, fw)], sem_d_s.at[wave, i])
            return 0

        lax.fori_loop(1, ep, sent_dispatch, 0)

        @pl.when(c != own_half)
        def _():
            left(outbound.at[pl.ds(0, SLOTS), pl.ds(0, fw)], sem_d_s.at[wave, 0])

    for i in range(1, nx):
        q_copy(i).wait_send()
        o_copy(i).wait_send()
    for way, m in [(1, 0), (-1, 0)] + chain:
        if kv_passes(way, m):
            kv_pass(way, m).wait_send()
        if m:
            kv_twin(way, m).wait_send()
    for copy in extra:
        copy.wait_send()
    for s in range(half_y):
        w_ahead(s).wait_send()
        if s < half_y - 1:
            w_behind(s).wait_send()
        for way in range(2):
            for k in range(CHUNKS):
                if ring_has(way, s, k):
                    ring_copy(way, s, k).wait_send()
    for k in range(2):
        for wave in range(2):
            swap(k, wave).wait_send()
    for s in range(half_y + 1):
        for r in w_fresh(s):
            w_twin(r).wait_send()
            for k in range(2):
                w_swap(r, k).wait_send()
    w_far().wait_send()

    def sent_back(j, _):
        for core in range(2):
            here = (c * half_ep + j == me_e) & (c == core)

            @pl.when(jnp.logical_not(here))
            def _():
                left(rows_out.at[core, pl.ds(0, SLOTS)], sem_r_s.at[j, core])

        return 0

    lax.fori_loop(0, half_ep, sent_back, 0)

    def sent_a(i, _):
        left(att_out.at[pl.ds(0, ht)], sem_a_s.at[i])
        return 0

    lax.fori_loop(1, tp, sent_a, 0)


PLAN = (
    "own0", "kv0", "kv1", "w1", "own1", "attend0", "extra", "w2", "slots0", "attend1", "slots1", "wx",
    "kv2", "kv3", "ffn1", "kv4", "kv5", "w3", "ffn2", "ring0", "attend2", "kv6", "attend3", "ring1", "attend4",
    "attend5", "ring2", "attend6", "w4", "wx", "hot", "ring3", "attend_end", "ring_end", "w_end",
    "project", "combine",
)


def default_plan(half_y, shards):
    plan = []
    for word in PLAN:
        name, arg = word.rstrip("0123456789"), word.lstrip("abcdefghijklmnopqrstuvwxyz_")
        if name == "ffn":
            name, arg = word, 0
        if name in ("kv", "attend") and int(arg) >= shards or name == "w" and int(arg) > half_y:
            continue
        if name == "ring" and int(arg) >= half_y:
            continue
        plan.append((name, int(arg or 0)))
    return plan


def local(g, queries, key_input, value_input, query_gain, key_gain, mix_out_weight, expert_input, ffn_gain,
          routes, route_scores, gate_weight, up_weight, down_weight):
    ep, tp = g.nz * g.nx, g.ny * 2
    tables = angle_tables(ep * g.tq // GRID_W)
    half_slots = ep // 2 * SLOTS
    vmem = pl.BlockSpec(memory_space=pltpu.VMEM)
    hbm = pl.BlockSpec(memory_space=pl.ANY)
    yb = g.d // g.ny
    half_y = g.ny // 2
    dma = pltpu.SemaphoreType.DMA
    return pl.pallas_call(
        functools.partial(kernel, g),
        out_shape=(
            jax.ShapeDtypeStruct((g.tq // tp, g.d), BF16),
            jax.ShapeDtypeStruct((g.tok, g.d // tp), BF16),
        ),
        in_specs=[hbm] * 17,
        out_specs=(vmem, vmem),
        scratch_shapes=[
            pltpu.VMEM((g.nz, g.tq, 2 * HD), BF16),
            pltpu.VMEM((HD, g.tq), BF16),
            pltpu.VMEM((g.nx, HD, g.tq), BF16),
            pltpu.VMEM((g.nx, 80, g.tq), F32),
            pltpu.VMEM((g.nx, 80, g.tq), BF16),
            pltpu.VMEM((g.nx, 80, g.tq), BF16),
            pltpu.VMEM((g.tq // 2, 2 * HD), BF16),
            pltpu.VMEM((g.tq // 2, 2 * HD), BF16),
            pltpu.VMEM((g.tq, 2 * HD), F32),
            pltpu.VMEM((g.ny, 2, HD, g.d), BF16),
            pltpu.VMEM((g.tok, g.d // 4), BF16),
            pltpu.VMEM((ep * SLOTS, g.d // 4), BF16),
            pltpu.VMEM((half_slots, g.d), BF16),
            pltpu.VMEM((2, g.d, g.ff), BF16),
            pltpu.VMEM((2, g.d, g.ff), BF16),
            pltpu.VMEM((2 * g.ff, g.d), BF16),
            pltpu.VMEM((2, half_slots, g.ff), F32),
            pltpu.VMEM((2, half_slots, g.ff), F32),
            pltpu.VMEM((half_slots, 128), F32),
            pltpu.VMEM((half_slots, 2 * g.ff), BF16),
            pltpu.VMEM((2, half_y, half_slots, yb), BF16),
            pltpu.VMEM((2, half_y, half_slots, yb), BF16),
            pltpu.VMEM((2, half_slots, yb // 2), BF16),
            pltpu.VMEM((ep * SLOTS, yb // 2), BF16),
            pltpu.VMEM((2, g.tok_pad, ep * SLOTS), BF16),
            pltpu.VMEM((2, g.tok_pad, 128), F32),
            pltpu.VMEM((2, 2, half_slots, yb), F32),
            pltpu.VMEM((HD, g.tq), BF16),
            pltpu.VMEM((g.tq, 2 * HD), BF16),
            pltpu.VMEM((g.tq, 2 * HD), BF16),
            pltpu.VMEM((1, HD), F32),
            pltpu.VMEM((1, HD), F32),
            pltpu.VMEM((g.tq // GRID_W, 2 * HD), F32),
            pltpu.VMEM((g.tq // GRID_W, 2 * HD), F32),
            pltpu.VMEM((GRID_W, 2 * HD), F32),
            pltpu.VMEM((GRID_W, 2 * HD), F32),
            pltpu.VMEM((2, g.tok), jnp.int32),
            pltpu.VMEM((2, g.tok), F32),
            pltpu.VMEM((1, g.d), F32),
            dma((17,)),
            dma((2, g.nz // 2)), dma((g.nz,)), dma((g.nz,)), dma((g.nz,)),
            dma((g.nx,)), dma((g.nx,)), dma((g.nx,)), dma((g.nx,)),
            dma((tp,)), dma((tp,)),
            dma((2, half_y)), dma((2, half_y)), dma((g.ny + 1,)), dma((g.ny + 1,)), dma((2, g.ny)), dma((2, g.ny)),
            dma((3,)), dma((3,)),
            dma((2, ep)), dma((2, ep)),
            dma((2, 2)), dma((2, 2)),
            dma((2, half_y, CHUNKS)), dma((2, half_y, CHUNKS)),
            dma((ep // 2, 2)), dma((ep,)),
        ],
        compiler_params=pltpu.CompilerParams(
            collective_id=0, has_side_effects=True, vmem_limit_bytes=62 * 1024 * 1024
        ),
    )(
        queries.T, key_input, value_input, key_gain.reshape(1, HD), query_gain.reshape(1, HD),
        *[jnp.asarray(t) for t in tables],
        expert_input, routes.T, route_scores.T, ffn_gain.reshape(1, g.d), mix_out_weight,
        gate_weight, up_weight, down_weight,
    )


SIZES = SimpleNamespace(nz=8, nx=4, ny=8, tq=512, tok=160, tok_pad=256, d=2048, ff=256, kv_heads=4, plan=default_plan)


def solution(mesh, g=SIZES):
    placed = (
        P("ep", "tp"),
        P("ep", None),
        P("ep", None),
        P(),
        P(),
        P("tp", None),
        P("ep", None),
        P(),
        P("ep", None),
        P("ep", None),
        P("ep", None, "tp"),
        P("ep", None, "tp"),
        P("ep", "tp", None),
    )
    return jax.shard_map(
        functools.partial(local, g),
        mesh=mesh,
        in_specs=placed,
        out_specs=(P(("ep", "tp"), None), P("ep", "tp")),
        check_vma=False,
    )
```

```python
import contextlib
import functools
import math
from types import SimpleNamespace

import jax
import jax.numpy as jnp
import numpy as np
from jax import lax
from jax.experimental import pallas as pl
from jax.experimental.pallas import tpu as pltpu
from jax.sharding import PartitionSpec as P

HD = 64
GRID_W = 64
EPSILON = 1e-06
ROPE_BASE = 10000.0
SLOTS = 16
CHUNKS = 4
MESH = pl.DeviceIdType.MESH
F32 = jnp.float32
BF16 = jnp.bfloat16
TRACE = False


def scope(name):
    return jax.named_scope(name) if TRACE else contextlib.nullcontext()


def angle_tables(rows):
    quarter = HD // 4
    inverse = (ROPE_BASE ** (-np.arange(quarter, dtype=np.float32) / quarter)).astype(np.float32)
    lane = np.arange(2 * HD)
    freq = inverse[lane % quarter]
    is_row = (lane % HD) < HD // 2
    sign = np.where((lane // quarter) % 2 == 0, -1.0, 1.0).astype(np.float32)

    def table(count, keep):
        angle = (np.arange(count, dtype=np.float32)[:, None] * freq[None, :]).astype(np.float32)
        cos = np.where(keep, np.cos(angle), 0.0).astype(np.float32)
        sin = np.where(keep, np.sin(angle) * sign, 0.0).astype(np.float32)
        return cos, sin

    return table(rows, is_row) + table(GRID_W, ~is_row)


def kernel(
    g,
    queries_h,
    keys_h,
    values_h,
    key_gain_h,
    query_gain_h,
    row_cos_h,
    row_sin_h,
    col_cos_h,
    col_sin_h,
    tokens,
    routes_h,
    scores_h,
    ffn_gain_h,
    mix_w,
    gate_w,
    up_w,
    down_w,
    mixed_out,
    expert_out,
    kv,
    q_own,
    q_all,
    o_acc,
    o_out,
    o_in,
    att_out,
    att_in,
    att_row,
    w_all,
    tok_own,
    outbound,
    slots,
    wg,
    wu,
    wd,
    gate_acc,
    up_acc,
    sq_acc,
    hidden,
    ring_out,
    ring_in,
    rows_out,
    rows_in,
    hot,
    share,
    ring_part,
    q_raw,
    k_raw,
    v_raw,
    key_gain,
    query_gain,
    row_cos,
    row_sin,
    col_cos,
    col_sin,
    routes,
    scores,
    ffn_gain,
    sem_local,
    sem_kv_s,
    sem_kv_r,
    sem_kvf_s,
    sem_kvf_r,
    sem_q_s,
    sem_q_r,
    sem_o_s,
    sem_o_r,
    sem_a_s,
    sem_a_r,
    sem_w_s,
    sem_w_r,
    sem_wf_s,
    sem_wf_r,
    sem_wx_s,
    sem_wx_r,
    sem_ex_s,
    sem_ex_r,
    sem_d_s,
    sem_d_r,
    sem_b_s,
    sem_b_r,
    sem_c_s,
    sem_c_r,
    sem_r_s,
    sem_r_r,
):
    nz, nx, ny, ep, tp = g.nz, g.nx, g.ny, g.nz * g.nx, g.ny * 2
    half_ep = ep // 2
    me_e, me_t = lax.axis_index("ep"), lax.axis_index("tp")
    z, x = me_e // nx, me_e % nx
    y, c = me_t // 2, me_t % 2
    sib = me_t + 1 - 2 * c
    own_half = me_e // half_ep
    tq, tok, d, ff = g.tq, g.tok, g.d, g.ff
    feat = d // 4
    par = y % 2

    def send(src, dst, ssem, rsem, to_e, to_t):
        return pltpu.make_async_remote_copy(
            src_ref=src, dst_ref=dst, send_sem=ssem, recv_sem=rsem,
            device_id=(to_e, to_t), device_id_type=MESH,
        )

    def arrived(dst, rsem):
        send(dst, dst, rsem, rsem, me_e, sib).wait_recv()

    def left(src, ssem):
        send(src, src, ssem, ssem, me_e, sib).wait_send()

    def al(v, m):
        return pl.multiple_of(v, m)

    barrier = pltpu.get_barrier_semaphore()

    def greet_plane(i, _):
        pl.semaphore_signal(barrier, inc=1, device_id=((me_e + i) % ep, me_t), device_id_type=MESH)
        pl.semaphore_signal(barrier, inc=1, device_id=((me_e + i) % ep, sib), device_id_type=MESH)
        return 0

    def greet_line(i, _):
        pl.semaphore_signal(barrier, inc=1, device_id=(me_e, (me_t + i) % tp), device_id_type=MESH)
        return 0

    lax.fori_loop(1, ep, greet_plane, 0)
    lax.fori_loop(1, tp, greet_line, 0)

    feat_at = al((par * 2 + c) * feat, feat)
    dh = d // 2
    col_half = x % 2
    cols_mine = pl.ds(al(col_half * dh, dh), dh)
    cols_other = pl.ds(al((1 - col_half) * dh, dh), dh)
    blocks = tq // GRID_W
    head = me_t * g.kv_heads // tp
    head_at = al((head // 2) * 2 * HD, 2 * HD) if g.kv_heads > 1 else 0
    head_lanes = pl.ds(head_at, 2 * HD) if g.kv_heads > 1 else pl.ds(0, HD)
    kv_lanes = slice(0, 2 * HD) if g.kv_heads > 1 else slice(0, HD)
    pairs = [
        (routes_h, routes),
        (scores_h, scores),
        (tokens.at[:, pl.ds(feat_at, feat)], tok_own),
        (queries_h, q_raw),
        (keys_h.at[:, head_lanes], k_raw.at[:, kv_lanes]),
        (values_h.at[:, head_lanes], v_raw.at[:, kv_lanes]),
        (key_gain_h, key_gain),
        (query_gain_h, query_gain),
        (row_cos_h.at[pl.ds(me_e * blocks, blocks)], row_cos),
        (row_sin_h.at[pl.ds(me_e * blocks, blocks)], row_sin),
        (col_cos_h, col_cos),
        (col_sin_h, col_sin),
        (mix_w.at[:, cols_mine], w_all.at[y, c, :, cols_mine]),
        (gate_w.at[0], wg.at[c]),
        (up_w.at[0], wu.at[c]),
        (down_w.at[0], wd.at[pl.ds(al(c * ff, ff), ff)]),
        (ffn_gain_h, ffn_gain),
    ]
    loads = [pltpu.make_async_copy(a, b, sem_local.at[i]) for i, (a, b) in enumerate(pairs)]
    for copy in loads:
        copy.start()

    for copy in loads[0:2]:
        copy.wait()
    r0, r1 = routes[0:1, :], routes[1:2, :]
    rows_e = lax.broadcasted_iota(jnp.int32, (ep, tok), 0)
    hit0 = (rows_e == r0).astype(F32)
    hit1 = (rows_e == r1).astype(F32)
    before = (
        lax.broadcasted_iota(jnp.int32, (tok, tok), 0) < lax.broadcasted_iota(jnp.int32, (tok, tok), 1)
    ).astype(BF16)
    count = jnp.dot((hit0 + hit1).astype(BF16), before, preferred_element_type=F32)
    slot0 = r0 * SLOTS + jnp.sum(count * hit0, axis=0, keepdims=True).astype(jnp.int32)
    slot1 = r1 * SLOTS + jnp.sum(count * hit1, axis=0, keepdims=True).astype(jnp.int32)
    rows_s = lax.broadcasted_iota(jnp.int32, (ep * SLOTS, tok), 0)
    to_slots = ((rows_s == slot0) | (rows_s == slot1)).astype(BF16)
    loads[2].wait()
    outbound[...] = jnp.dot(to_slots, tok_own[...], preferred_element_type=F32).astype(BF16)

    lane = lax.broadcasted_iota(jnp.int32, (GRID_W, 2 * HD), 1)
    low = lane < HD
    is_u = (lane // (HD // 4)) % 2 == 0
    for copy in loads[3:12]:
        copy.wait()
    gain = jnp.concatenate([key_gain[...], query_gain[...]], axis=1)
    odd = head % 2 == 1
    q_wide = jnp.transpose(jnp.concatenate([q_raw[...], q_raw[...]], axis=0).astype(F32))
    if g.kv_heads > 1:
        k_all, v_all = k_raw[...].astype(F32), v_raw[...].astype(F32)
        k_wide = jnp.where(odd, pltpu.roll(k_all, HD, 1), k_all)
        v_wide = jnp.where(odd, v_all, pltpu.roll(v_all, HD, 1))
    else:
        k_wide = jnp.concatenate([k_raw[:, 0:HD]] * 2, axis=1).astype(F32)
        v_wide = jnp.concatenate([v_raw[:, 0:HD]] * 2, axis=1).astype(F32)
    for b in range(blocks):
        at = b * GRID_W
        v = jnp.where(low, k_wide[at : at + GRID_W], q_wide[at : at + GRID_W])
        sq = v * v
        s_low = jnp.sum(jnp.where(low, sq, 0.0), axis=1, keepdims=True)
        s_high = jnp.sum(jnp.where(low, 0.0, sq), axis=1, keepdims=True)
        scale = jnp.where(low, lax.rsqrt(s_low * (1.0 / HD) + EPSILON), lax.rsqrt(s_high * (1.0 / HD) + EPSILON))
        n = v * scale * gain
        cos = col_cos[...] + row_cos[b : b + 1, :]
        sin = col_sin[...] + row_sin[b : b + 1, :]
        swapped = jnp.where(is_u, pltpu.roll(n, 2 * HD - HD // 4, 1), pltpu.roll(n, HD // 4, 1))
        turned = n * cos + swapped * sin
        kv[z, at : at + GRID_W, :] = jnp.where(low, turned, v_wide[at : at + GRID_W]).astype(BF16)
        att_row[at : at + GRID_W, :] = turned
    q_own[...] = jnp.transpose(att_row[...])[HD : 2 * HD, :].astype(BF16)

    with scope("barrier"):
        pl.semaphore_wait(barrier, 2 * (ep - 1) + tp - 1)

    slot_at = al((me_e % half_ep) * SLOTS, SLOTS)
    to_core = y * 2 + own_half

    fw = feat // 2

    def wave_lanes(wave):
        return pl.ds(wave * fw, fw), pl.ds(al(feat_at + wave * fw, fw), fw)

    def dispatch(i, wave):
        to_e = (me_e + i) % ep
        return send(
            outbound.at[pl.ds(al(to_e * SLOTS, SLOTS), SLOTS), wave_lanes(wave)[0]],
            slots.at[pl.ds(slot_at, SLOTS), wave_lanes(wave)[1]],
            sem_d_s.at[wave, i], sem_d_r.at[wave, (me_e % half_ep) * 2 + c], to_e, to_core,
        )

    def dispatch_self(wave):
        return pltpu.make_async_copy(
            outbound.at[pl.ds(al(me_e * SLOTS, SLOTS), SLOTS), wave_lanes(wave)[0]],
            slots.at[pl.ds(slot_at, SLOTS), wave_lanes(wave)[1]],
            sem_d_r.at[wave, (me_e % half_ep) * 2 + c],
        )

    def q_copy(i):
        return send(q_own, q_all.at[x], sem_q_s.at[i], sem_q_r.at[x], z * nx + (x + i) % nx, me_t)

    q_all[x] = q_own[...]
    for i in range(1, nx):
        q_copy(i).start()

    hq = tq // 2
    kv_mine = pl.ds(al(c * hq, hq), hq)
    kv_other = pl.ds(al((1 - c) * hq, hq), hq)

    half_z = nz // 2
    way_c = 1 - 2 * c
    chain = [(way, m) for m in range(1, half_z + 1) for way in (1, -1) if way == 1 or m < half_z]

    def shard(way, m):
        return (z + nz - way * way_c * m) % nz

    def kv_pass(way, m):
        b = kv.at[shard(way, m), kv_mine]
        to_z = (z + nz + way * way_c) % nz
        at = 0 if way == 1 else 1
        return send(b, b, sem_kv_s.at[at, m], sem_kv_r.at[shard(way, m)], to_z * nx + x, me_t)

    def kv_passes(way, m):
        return m < half_z if way == 1 else m < half_z - 1

    for way in (1, -1):
        if kv_passes(way, 0):
            kv_pass(way, 0).start()

    near = ep // 4
    for wave in range(2):

        def dispatch_start(i, _):
            dispatch(i, wave).start()
            return 0

        lax.fori_loop(near, ep - near, dispatch_start, 0)
        lax.fori_loop(1, near, dispatch_start, 0)
        lax.fori_loop(ep - near, ep, dispatch_start, 0)

        @pl.when(c == own_half)
        def _():
            dispatch_self(wave).start()

        @pl.when(c != own_half)
        def _():
            dispatch(0, wave).start()

    for copy in loads[12:]:
        copy.wait()

    extra = [
        send(wg.at[c], wg.at[c], sem_ex_s.at[0], sem_ex_r.at[0], me_e, sib),
        send(wu.at[c], wu.at[c], sem_ex_s.at[1], sem_ex_r.at[1], me_e, sib),
        send(
            wd.at[pl.ds(al(c * ff, ff), ff)], wd.at[pl.ds(al(c * ff, ff), ff)],
            sem_ex_s.at[2], sem_ex_r.at[2], me_e, sib,
        ),
    ]

    def extra_start():
        for copy in extra:
            copy.start()

    half_y = ny // 2
    right = ((y + 1) % ny) * 2 + c
    leftward = ((y + ny - 1) % ny) * 2 + c
    ahead = ((y + ny + way_c) % ny) * 2 + c
    behind = ((y + ny - way_c) % ny) * 2 + c

    def w_block(s):
        return w_all.at[(y + ny + ny - way_c * s) % ny, c, :, cols_mine]

    def w_ahead(s):
        return send(w_block(s), w_block(s), sem_w_s.at[0, s], sem_w_r.at[0, s], me_e, ahead)

    def w_behind(s):
        return send(w_block(-s), w_block(-s), sem_w_s.at[1, s], sem_w_r.at[1, s], me_e, behind)

    def w_fresh(s):
        return [s] if s in (0, half_y) else [s, -s]

    def w_row(r):
        return (y + ny + ny - way_c * r) % ny

    def w_quarter(r, k, other):
        half = 1 - col_half if other else col_half
        return w_all.at[w_row(r), c, :, pl.ds(al(half * dh + k * (dh // 2), dh // 2), dh // 2)]

    def w_swap(r, k):
        to_x = (x + nx - 1) % nx if k == 0 else (x + 1) % nx
        q = w_quarter(r, k, False)
        return send(q, q, sem_wx_s.at[k, w_row(r)], sem_wx_r.at[k, w_row(r)], z * nx + to_x, me_t)

    def w_twin(r):
        b = w_block(r)
        return send(b, b, sem_wf_s.at[w_row(r)], sem_wf_r.at[w_row(r)], me_e, sib)

    def w_step(s):
        if s > 0:
            arrived(w_block(s), sem_w_r.at[0, s - 1])
            if s < half_y:
                arrived(w_block(-s), sem_w_r.at[1, s - 1])
        if s < half_y:
            w_ahead(s).start()
        if s < half_y - 1:
            w_behind(s).start()
        pending.extend(w_fresh(s))

    pending = []

    def w_exchange():
        for r in pending:
            for k in range(2):
                w_swap(r, k).start()
            w_twin(r).start()
        pending.clear()

    def w_far():
        b = w_all.at[:, c, :, cols_other]
        return send(b, b, sem_wf_s.at[ny], sem_wf_r.at[ny], me_e, sib)

    def w_end():
        for s in range(half_y + 1):
            for r in w_fresh(s):
                for k in range(2):
                    arrived(w_quarter(r, k, True), sem_wx_r.at[k, w_row(r)])
        w_far().start()

    def o_copy(j):
        to_x = (x + j) % nx
        return send(o_out.at[to_x], o_in.at[x], sem_o_s.at[j], sem_o_r.at[x], z * nx + to_x, me_t)

    score_scale = HD ** (-0.5) * math.log2(math.e)

    def kv_twin(way, m):
        zz = shard(way, m)
        return send(kv.at[zz, kv_mine], kv.at[zz, kv_mine], sem_kvf_s.at[zz], sem_kvf_r.at[zz], me_e, sib)

    def kv_ready(i):
        way, m = chain[i]
        zz = shard(way, m)
        arrived(kv.at[zz, kv_mine], sem_kv_r.at[zz])
        if kv_passes(way, m):
            kv_pass(way, m).start()
        kv_twin(way, m).start()

    def values_of(zz):
        rows = lax.broadcasted_iota(jnp.int32, (80, tq), 0)
        return jnp.where(rows < 16, 1.0, jnp.transpose(kv[zz].astype(F32))[48:128, :]).astype(BF16)

    def scores_of(zz, vt, xx):
        s_t = jnp.dot(kv[zz, :, 0:HD], q_all[xx], preferred_element_type=F32)
        p = jnp.exp2(s_t * score_scale).astype(BF16)
        return jnp.dot(vt, p, preferred_element_type=F32)

    def attend_own(part):
        vt = values_of(z)
        for j in range(nx) if part is None else ([0] if part == 0 else range(1, nx)):
            xx = (x + j) % nx
            if j:
                arrived(q_all.at[xx], sem_q_r.at[xx])
            o_acc[xx] = scores_of(z, vt, xx)

    def attend(i):
        last = i == len(chain) - 1
        zz = shard(*chain[i])
        arrived(kv.at[zz, kv_other], sem_kvf_r.at[zz])
        vt = values_of(zz)
        for j in [nx // 2] + [j for j in range(1, nx + 1) if j != nx // 2]:
            xx = (x + j) % nx
            whole = o_acc[xx] + scores_of(zz, vt, xx)
            if last and j < nx:
                high = whole[0:8].astype(BF16)
                o_out[xx, 0:8] = high
                o_out[xx, 8:16] = (whole[8:16] - high.astype(F32)).astype(BF16)
                o_out[xx, 16:80] = whole[16:80].astype(BF16)
                o_copy(j).start()
            else:
                o_acc[xx] = whole

    own_at, other_at = par * (d // 2), (1 - par) * (d // 2)

    def swap(k, wave):
        at = al(own_at + k * feat + wave * fw, fw)
        b = slots.at[:, pl.ds(at, fw)]
        return send(b, b, sem_b_s.at[k, wave], sem_b_r.at[k, wave], me_e, leftward if k == 0 else right)

    def slots_ready(wave):
        for core in range(2):
            at = al(own_at + core * feat + wave * fw, fw)

            def one(j, _):
                arrived(
                    slots.at[pl.ds(al(j * SLOTS, SLOTS), SLOTS), pl.ds(at, fw)], sem_d_r.at[wave, j * 2 + core]
                )
                return 0

            lax.fori_loop(0, half_ep, one, 0)
            swap(core, wave).start()

    def half_products(start, first):
        for k in range(2):
            at = al(start + k * feat, feat)
            v = slots[:, pl.ds(at, feat)].astype(F32)
            sq = jnp.sum(v * v, axis=1, keepdims=True)
            scaled = (v * ffn_gain[:, pl.ds(at, feat)]).astype(BF16)
            for core in range(2):
                gp = jnp.dot(scaled, wg[core, pl.ds(at, feat), :], preferred_element_type=F32)
                up = jnp.dot(scaled, wu[core, pl.ds(at, feat), :], preferred_element_type=F32)
                if first and k == 0:
                    gate_acc[core], up_acc[core] = gp, up
                else:
                    gate_acc[core], up_acc[core] = gate_acc[core] + gp, up_acc[core] + up
            if first and k == 0:
                sq_acc[...] = jnp.broadcast_to(sq, sq_acc.shape)
            else:
                sq_acc[...] = sq_acc[...] + sq

    def ffn_first():
        for k in range(2):
            arrived(wg.at[1 - c], sem_ex_r.at[0]) if k == 0 else arrived(wu.at[1 - c], sem_ex_r.at[1])
        arrived(wd.at[pl.ds(al((1 - c) * ff, ff), ff)], sem_ex_r.at[2])
        half_products(own_at, True)

    def ffn_second():
        for k in range(2):
            for wave in range(2):
                arrived(slots.at[:, pl.ds(al(other_at + k * feat + wave * fw, fw), fw)], sem_b_r.at[k, wave])
        half_products(other_at, False)
        scale = lax.rsqrt(sq_acc[:, 0:1] * (1.0 / d) + EPSILON)
        for core in range(2):
            gate = scale * gate_acc[core]
            hidden[:, core * ff : (core + 1) * ff] = (
                gate / (1.0 + jnp.exp(-gate)) * (scale * up_acc[core])
            ).astype(BF16)
        ring_fill(0)

    yb = d // ny
    n_slots = half_ep * SLOTS
    hs = n_slots // 2

    def partial_of(dest):
        return jnp.dot(hidden[...], wd[:, pl.ds(al(dest * yb, yb), yb)], preferred_element_type=F32)

    cr = n_slots // CHUNKS

    def ring_has(way, s, k):
        return s > 0 or (k < CHUNKS // 2) == (way == 0)

    def ring_copy(way, s, k):
        rows = pl.ds(k * cr, cr)
        return send(
            ring_out.at[way, s, rows], ring_in.at[way, s, rows], sem_c_s.at[way, s, k], sem_c_r.at[way, s, k],
            me_e, right if way == 0 else leftward,
        )

    def ring_take(way, s, k, block):
        if not ring_has(way, s, k):
            return block
        rows = slice(k * cr, (k + 1) * cr)
        arrived(ring_in.at[way, s, pl.ds(k * cr, cr)], sem_c_r.at[way, s, k])
        return block + ring_in[way, s, rows].astype(F32)

    def ring_fill(s):
        for way in range(1 if s in (0, half_y) else 2):
            dest = (y + half_y - s) % ny if way == 0 else (y + ny - half_y + s) % ny
            ring_part[s % 2, way] = partial_of(dest)

    def ring_step(s):
        for j in range(CHUNKS):
            for way in range(2):
                k = (j + CHUNKS // 2) % CHUNKS if (s == 1 and way == 0) or (s != 1 and way == 1) else j
                if not ring_has(way, s, k):
                    continue
                rows = slice(k * cr, (k + 1) * cr)
                block = ring_part[s % 2, way if s else 0, rows]
                if s:
                    block = ring_take(way, s - 1, k, block)
                ring_out[way, s, rows] = block.astype(BF16)
                ring_copy(way, s, k).start()
        ring_fill(s + 1)

    def back_copy(j, core):
        src_e = c * half_ep + j
        return send(
            rows_out.at[core, pl.ds(al(j * SLOTS, SLOTS), SLOTS)],
            rows_in.at[pl.ds(al(me_e * SLOTS, SLOTS), SLOTS)],
            sem_r_s.at[j, core], sem_r_r.at[me_e], src_e, y * 2 + core,
        )

    def back_self(j, core):
        return pltpu.make_async_copy(
            rows_out.at[core, pl.ds(al(j * SLOTS, SLOTS), SLOTS)],
            rows_in.at[pl.ds(al(me_e * SLOTS, SLOTS), SLOTS)],
            sem_r_r.at[me_e],
        )

    def ring_end():
        s = half_y - 1

        def one(j, _):
            for core in range(2):
                here = (c * half_ep + j == me_e) & (c == core)

                @pl.when(here)
                def _():
                    back_self(j, core).start()

                @pl.when(jnp.logical_not(here))
                def _():
                    back_copy(j, core).start()

            return 0

        for k in range(CHUNKS):
            rows = slice(k * cr, (k + 1) * cr)
            block = ring_part[half_y % 2, 0, rows]
            for way in range(2):
                block = ring_take(way, s, k, block)
            block = block.astype(BF16)
            for core in range(2):
                rows_out[core, rows] = block[:, core * (yb // 2) : (core + 1) * (yb // 2)]
            per = half_ep // CHUNKS
            lax.fori_loop(k * per, (k + 1) * per, one, 0)

    def make_hot():
        fill = jnp.full((1, g.tok_pad - tok), -1, jnp.int32)
        rows = lax.broadcasted_iota(jnp.int32, (ep * SLOTS, g.tok_pad), 0)
        w0, w1 = scores[0:1, :], scores[1:2, :]
        whole = w0 + w1
        for k, (slot, w) in enumerate(((slot0, w0 / whole), (slot1, w1 / whole))):
            mask = (rows == jnp.concatenate([slot, fill], axis=1)).astype(F32)
            hot[k] = jnp.transpose(mask).astype(BF16)
            wide = jnp.concatenate([w, jnp.zeros((1, g.tok_pad - tok), F32)], axis=1)
            share[k] = jnp.transpose(jnp.broadcast_to(wide, (128, g.tok_pad)))

    def combine():
        def one(j, _):
            arrived(rows_in.at[pl.ds(al(j * SLOTS, SLOTS), SLOTS)], sem_r_r.at[j])
            return 0

        lax.fori_loop(0, ep, one, 0)
        p0 = jnp.dot(hot[0], rows_in[...], preferred_element_type=F32)
        p1 = jnp.dot(hot[1], rows_in[...], preferred_element_type=F32)
        expert_out[...] = (p0 * share[0] + p1 * share[1])[0:tok].astype(BF16)

    rows_t = tq // tp
    ht = rows_t // 2

    def a_copy(i):
        to_t = (me_t + i) % tp
        return send(
            att_out.at[pl.ds(al(to_t * ht, ht), ht)], att_in.at[pl.ds(al(me_t * ht, ht), ht)],
            sem_a_s.at[i], sem_a_r.at[me_t], me_e, to_t,
        )

    a_self = pltpu.make_async_copy(
        att_out.at[pl.ds(al(me_t * ht, ht), ht)], att_in.at[pl.ds(al(me_t * ht, ht), ht)], sem_a_r.at[me_t]
    )

    def attend_end():
        total = o_acc[x]
        numer, denom = total[16:80], total[0:8]
        for i in range(1, nx):
            xx = (x + i) % nx
            arrived(o_in.at[xx], sem_o_r.at[xx])
            numer = numer + o_in[xx, 16:80].astype(F32)
            denom = denom + o_in[xx, 0:8].astype(F32) + o_in[xx, 8:16].astype(F32)
        att_t = numer / denom[0:1]
        att = jnp.transpose(jnp.concatenate([att_t, att_t], axis=0))[:, 0:HD]
        for t in range(tp):
            at = t * rows_t
            att_out[t * ht : (t + 1) * ht, :] = jnp.concatenate(
                [att[at : at + ht], att[at + ht : at + rows_t]], axis=1
            ).astype(BF16)
        a_self.start()

        def one(i, _):
            a_copy(i).start()
            return 0

        lax.fori_loop(1, tp, one, 0)

    def project():
        def one(j, _):
            arrived(att_in.at[pl.ds(al(j * ht, ht), ht)], sem_a_r.at[j])
            return 0

        lax.fori_loop(0, tp, one, 0)

        for yy in range(ny):
            arrived(w_all.at[yy, 1 - c, :, cols_mine], sem_wf_r.at[yy])
        arrived(w_all.at[:, 1 - c, :, cols_other], sem_wf_r.at[ny])
        pieces = []
        for j in range(tp // 2):
            a = att_in[2 * j * ht : (2 * j + 1) * ht, :]
            b = att_in[(2 * j + 1) * ht : (2 * j + 2) * ht, :]
            top = jnp.concatenate([a[:, 0:HD], b[:, 0:HD]], axis=1)
            low_rows = jnp.concatenate([a[:, HD:], b[:, HD:]], axis=1)
            pieces.append(jnp.concatenate([top, low_rows], axis=0))
        lhs = jnp.concatenate(pieces, axis=1)
        mixed_out[...] = jnp.dot(lhs, w_all[...].reshape(tp * HD, d), preferred_element_type=F32).astype(BF16)

    w_step(0)
    plan = g.plan(half_y, len(chain))
    actions = dict(
        ffn1=ffn_first, ffn2=ffn_second, ring_end=ring_end,
        attend_end=attend_end, project=project, combine=combine, hot=make_hot, w_end=w_end, extra=extra_start, wx=w_exchange,
    )
    for name, arg in plan:
        with scope(name + str(arg)):
            if name == "kv":
                kv_ready(arg)
            elif name == "attend":
                attend(arg)
            elif name == "w":
                w_step(arg)
            elif name == "ring":
                ring_step(arg)
            elif name == "own":
                attend_own(arg)
            elif name == "slots":
                slots_ready(arg)
            else:
                actions[name]()

    for wave in range(2):

        def sent_dispatch(i, _):
            left(outbound.at[pl.ds(0, SLOTS), pl.ds(0, fw)], sem_d_s.at[wave, i])
            return 0

        lax.fori_loop(1, ep, sent_dispatch, 0)

        @pl.when(c != own_half)
        def _():
            left(outbound.at[pl.ds(0, SLOTS), pl.ds(0, fw)], sem_d_s.at[wave, 0])

    for i in range(1, nx):
        q_copy(i).wait_send()
        o_copy(i).wait_send()
    for way, m in [(1, 0), (-1, 0)] + chain:
        if kv_passes(way, m):
            kv_pass(way, m).wait_send()
        if m:
            kv_twin(way, m).wait_send()
    for copy in extra:
        copy.wait_send()
    for s in range(half_y):
        w_ahead(s).wait_send()
        if s < half_y - 1:
            w_behind(s).wait_send()
        for way in range(2):
            for k in range(CHUNKS):
                if ring_has(way, s, k):
                    ring_copy(way, s, k).wait_send()
    for k in range(2):
        for wave in range(2):
            swap(k, wave).wait_send()
    for s in range(half_y + 1):
        for r in w_fresh(s):
            w_twin(r).wait_send()
            for k in range(2):
                w_swap(r, k).wait_send()
    w_far().wait_send()

    def sent_back(j, _):
        for core in range(2):
            here = (c * half_ep + j == me_e) & (c == core)

            @pl.when(jnp.logical_not(here))
            def _():
                left(rows_out.at[core, pl.ds(0, SLOTS)], sem_r_s.at[j, core])

        return 0

    lax.fori_loop(0, half_ep, sent_back, 0)

    def sent_a(i, _):
        left(att_out.at[pl.ds(0, ht)], sem_a_s.at[i])
        return 0

    lax.fori_loop(1, tp, sent_a, 0)


PLAN = (
    "own0", "kv0", "kv1", "w1", "own1", "attend0", "extra", "w2", "slots0", "attend1", "slots1", "wx",
    "kv2", "kv3", "ffn1", "attend2", "kv4", "kv5", "w3", "ffn2", "ring0", "attend3", "kv6", "ring1", "attend4",
    "attend5", "ring2", "attend6", "hot", "w4", "wx", "ring3", "attend_end", "ring_end", "w_end",
    "project", "combine",
)


def default_plan(half_y, shards):
    plan = []
    for word in PLAN:
        name, arg = word.rstrip("0123456789"), word.lstrip("abcdefghijklmnopqrstuvwxyz_")
        if name == "ffn":
            name, arg = word, 0
        if name in ("kv", "attend") and int(arg) >= shards or name == "w" and int(arg) > half_y:
            continue
        if name == "ring" and int(arg) >= half_y:
            continue
        plan.append((name, int(arg or 0)))
    return plan


def local(g, queries, key_input, value_input, query_gain, key_gain, mix_out_weight, expert_input, ffn_gain,
          routes, route_scores, gate_weight, up_weight, down_weight):
    ep, tp = g.nz * g.nx, g.ny * 2
    tables = angle_tables(ep * g.tq // GRID_W)
    half_slots = ep // 2 * SLOTS
    vmem = pl.BlockSpec(memory_space=pltpu.VMEM)
    hbm = pl.BlockSpec(memory_space=pl.ANY)
    yb = g.d // g.ny
    half_y = g.ny // 2
    dma = pltpu.SemaphoreType.DMA
    return pl.pallas_call(
        functools.partial(kernel, g),
        out_shape=(
            jax.ShapeDtypeStruct((g.tq // tp, g.d), BF16),
            jax.ShapeDtypeStruct((g.tok, g.d // tp), BF16),
        ),
        in_specs=[hbm] * 17,
        out_specs=(vmem, vmem),
        scratch_shapes=[
            pltpu.VMEM((g.nz, g.tq, 2 * HD), BF16),
            pltpu.VMEM((HD, g.tq), BF16),
            pltpu.VMEM((g.nx, HD, g.tq), BF16),
            pltpu.VMEM((g.nx, 80, g.tq), F32),
            pltpu.VMEM((g.nx, 80, g.tq), BF16),
            pltpu.VMEM((g.nx, 80, g.tq), BF16),
            pltpu.VMEM((g.tq // 2, 2 * HD), BF16),
            pltpu.VMEM((g.tq // 2, 2 * HD), BF16),
            pltpu.VMEM((g.tq, 2 * HD), F32),
            pltpu.VMEM((g.ny, 2, HD, g.d), BF16),
            pltpu.VMEM((g.tok, g.d // 4), BF16),
            pltpu.VMEM((ep * SLOTS, g.d // 4), BF16),
            pltpu.VMEM((half_slots, g.d), BF16),
            pltpu.VMEM((2, g.d, g.ff), BF16),
            pltpu.VMEM((2, g.d, g.ff), BF16),
            pltpu.VMEM((2 * g.ff, g.d), BF16),
            pltpu.VMEM((2, half_slots, g.ff), F32),
            pltpu.VMEM((2, half_slots, g.ff), F32),
            pltpu.VMEM((half_slots, 128), F32),
            pltpu.VMEM((half_slots, 2 * g.ff), BF16),
            pltpu.VMEM((2, half_y, half_slots, yb), BF16),
            pltpu.VMEM((2, half_y, half_slots, yb), BF16),
            pltpu.VMEM((2, half_slots, yb // 2), BF16),
            pltpu.VMEM((ep * SLOTS, yb // 2), BF16),
            pltpu.VMEM((2, g.tok_pad, ep * SLOTS), BF16),
            pltpu.VMEM((2, g.tok_pad, 128), F32),
            pltpu.VMEM((2, 2, half_slots, yb), F32),
            pltpu.VMEM((HD, g.tq), BF16),
            pltpu.VMEM((g.tq, 2 * HD), BF16),
            pltpu.VMEM((g.tq, 2 * HD), BF16),
            pltpu.VMEM((1, HD), F32),
            pltpu.VMEM((1, HD), F32),
            pltpu.VMEM((g.tq // GRID_W, 2 * HD), F32),
            pltpu.VMEM((g.tq // GRID_W, 2 * HD), F32),
            pltpu.VMEM((GRID_W, 2 * HD), F32),
            pltpu.VMEM((GRID_W, 2 * HD), F32),
            pltpu.VMEM((2, g.tok), jnp.int32),
            pltpu.VMEM((2, g.tok), F32),
            pltpu.VMEM((1, g.d), F32),
            dma((17,)),
            dma((2, g.nz // 2)), dma((g.nz,)), dma((g.nz,)), dma((g.nz,)),
            dma((g.nx,)), dma((g.nx,)), dma((g.nx,)), dma((g.nx,)),
            dma((tp,)), dma((tp,)),
            dma((2, half_y)), dma((2, half_y)), dma((g.ny + 1,)), dma((g.ny + 1,)), dma((2, g.ny)), dma((2, g.ny)),
            dma((3,)), dma((3,)),
            dma((2, ep)), dma((2, ep)),
            dma((2, 2)), dma((2, 2)),
            dma((2, half_y, CHUNKS)), dma((2, half_y, CHUNKS)),
            dma((ep // 2, 2)), dma((ep,)),
        ],
        compiler_params=pltpu.CompilerParams(
            collective_id=0, has_side_effects=True, vmem_limit_bytes=62 * 1024 * 1024
        ),
    )(
        queries.T, key_input, value_input, key_gain.reshape(1, HD), query_gain.reshape(1, HD),
        *[jnp.asarray(t) for t in tables],
        expert_input, routes.T, route_scores.T, ffn_gain.reshape(1, g.d), mix_out_weight,
        gate_weight, up_weight, down_weight,
    )


SIZES = SimpleNamespace(nz=8, nx=4, ny=8, tq=512, tok=160, tok_pad=256, d=2048, ff=256, kv_heads=4, plan=default_plan)


def solution(mesh, g=SIZES):
    placed = (
        P("ep", "tp"),
        P("ep", None),
        P("ep", None),
        P(),
        P(),
        P("tp", None),
        P("ep", None),
        P(),
        P("ep", None),
        P("ep", None),
        P("ep", None, "tp"),
        P("ep", None, "tp"),
        P("ep", "tp", None),
    )
    return jax.shard_map(
        functools.partial(local, g),
        mesh=mesh,
        in_specs=placed,
        out_specs=(P(("ep", "tp"), None), P("ep", "tp")),
        check_vma=False,
    )
```
